128 devices in a mesh: rep: 2 (over z_hi), fs: 32 (over z_lo, y, x), tp: 2 (over core).
Axes of the slice: x: 4, y: 4, z: 4 (z_hi: 2, z_lo: 2; z = z_hi * 2 + z_lo), core: 2. Of those that a mesh axis runs over, the one named last changes fastest.
Arguments:
- tokens: bfloat16 [49152, 2048], P(('rep', 'fs', 'tp')), may hold values from -6 to 6
- outer_weight: float32 [2048, 1536], P('fs', 'tp'), may hold values from -0.125 to 0.125
- inner_weight: float32 [2048, 1536], P('fs', 'tp'), may hold values from -0.125 to 0.125
- value_weight: float32 [2048, 1536], P('fs', 'tp'), may hold values from -0.125 to 0.125
- conv_taps: float32 [3, 1536], P(None, 'tp'), may hold values from -3 to 3
- mix_out: float32 [1536, 2048], P('tp', 'fs'), may hold values from -0.15625 to 0.15625
- norm_first: float32 [2048], replicated, may hold values from 0.1 to 1.9
- up_weight: float32 [2048, 4096], P('fs', 'tp'), may hold values from -0.125 to 0.125
- down_weight: float32 [4096, 2048], P('tp', 'fs'), may hold values from -0.09375 to 0.09375
- norm_second: float32 [2048], replicated, may hold values from 0.1 to 1.9
Outputs:
- encoded: bfloat16 [49152, 2048], P(('rep', 'fs', 'tp'))
The draws below stay inside these ranges and needn't reach their ends.
All inputs are finite; a program needn't handle non-finite values.
Results may differ from the reference program's by a relative error of at most 0.015.
Values may be sent and summed in bfloat16 or wider, within the bound.
A program may use at most 128 MiB of HBM per device.

```python
import jax
import jax.numpy as jnp
from jax import lax

D = 2048
WA = 1536
FF = 4096
SEQ = 128
TOK_DEV = 384
TOKENS = 49152


def level_of(own_key, dims, split, least, top_value):
    gain, own = 1.0, jax.random.fold_in(own_key, 6)
    for axis_at, parts in split:
        steps = jnp.exp(jax.random.uniform(jax.random.fold_in(own, axis_at), (parts,), jnp.float32, least / len(split), top_value / len(split)))
        gain = gain * jnp.repeat(steps, dims[axis_at] // parts).reshape([-1 if axis == axis_at else 1 for axis in range(len(dims))])
    return gain


def gaussian(rng, dims, width, reach, split=(), kind=jnp.bfloat16):
    drawn = jax.random.normal(rng, dims, jnp.float32) * width
    if len(split) > 0:
        drawn = level_of(rng, dims, split, -0.22, 0.18) * drawn
    return jnp.clip(drawn, min=-reach, max=reach).astype(kind)


def setup_inputs(seed: int = 0) -> dict:
    arg_keys = jax.random.split(jax.random.key(seed), 11)
    tokens = gaussian(arg_keys[0], (TOKENS, D), 1.0, 6.0, ((0, 128),))
    outer_weight = gaussian(arg_keys[1], (D, WA), D ** -0.5, 0.125, ((0, 32), (1, 2)), jnp.float32)
    inner_weight = gaussian(arg_keys[2], (D, WA), D ** -0.5, 0.125, ((0, 32), (1, 2)), jnp.float32)
    value_weight = gaussian(arg_keys[3], (D, WA), D ** -0.5, 0.125, ((0, 32), (1, 2)), jnp.float32)
    conv_taps = gaussian(arg_keys[4], (3, WA), 0.6, 3.0, ((1, 2),), jnp.float32)
    mix_out = gaussian(arg_keys[5], (WA, D), WA ** -0.5, 0.15625, ((0, 2), (1, 32)), jnp.float32)
    norm_first = jnp.clip(1.0 + 0.18 * jax.random.normal(arg_keys[6], (D,), jnp.float32), 0.1, 1.9)
    up_weight = gaussian(arg_keys[7], (D, FF), D ** -0.5, 0.125, ((0, 32), (1, 2)), jnp.float32)
    down_weight = gaussian(arg_keys[8], (FF, D), FF ** -0.5, 0.09375, ((0, 2), (1, 32)), jnp.float32)
    norm_second = jnp.clip(1.0 + 0.18 * jax.random.normal(arg_keys[9], (D,), jnp.float32), 0.1, 1.9)
    return {"tokens": tokens, "outer_weight": outer_weight, "inner_weight": inner_weight, "value_weight": value_weight, "conv_taps": conv_taps, "mix_out": mix_out, "norm_first": norm_first, "up_weight": up_weight, "down_weight": down_weight, "norm_second": norm_second}


residual_scale = 2.0 ** 0.25
norm_epsilon = 1e-05

def layer_norm(values, scaling):
    center = values - lax.optimization_barrier(jnp.mean(values, axis=-1, keepdims=True))
    spread = lax.optimization_barrier(jnp.mean(center * center, axis=-1, keepdims=True))
    return center * lax.rsqrt(spread + norm_epsilon) * scaling

def reference(tokens, outer_weight, inner_weight, value_weight, conv_taps, mix_out, norm_first, up_weight, down_weight, norm_second):
    outer_bf = outer_weight.astype(jnp.bfloat16)
    inner_bf = inner_weight.astype(jnp.bfloat16)
    value_bf = value_weight.astype(jnp.bfloat16)
    mixout_bf = mix_out.astype(jnp.bfloat16)
    upward_bf = up_weight.astype(jnp.bfloat16)
    downward_bf = down_weight.astype(jnp.bfloat16)
    blocks = tokens.reshape(-1, TOK_DEV * 8, D)

    def one_block(rows):
        outer = jnp.dot(rows, outer_bf, preferred_element_type=jnp.float32)
        inner = jnp.dot(rows, inner_bf, preferred_element_type=jnp.float32)
        value = jnp.dot(rows, value_bf, preferred_element_type=jnp.float32)
        framed = (inner * value).reshape(-1, SEQ, WA)
        padded = jnp.pad(framed, ((0, 0), (1, 1), (0, 0)))
        convolved = padded[:, :-2] * conv_taps[0] + framed * conv_taps[1] + padded[:, 2:] * conv_taps[2]
        mixed = (outer * convolved.reshape(-1, WA)).astype(jnp.bfloat16)
        mixing = jnp.dot(mixed, mixout_bf, preferred_element_type=jnp.float32)
        first = layer_norm(residual_scale * rows.astype(jnp.float32) + mixing, norm_first).astype(jnp.bfloat16)
        raised = jax.nn.relu(jnp.dot(first, upward_bf, preferred_element_type=jnp.float32))
        hidden = (raised * raised).astype(jnp.bfloat16)
        lowered = jnp.dot(hidden, downward_bf, preferred_element_type=jnp.float32)
        return layer_norm(residual_scale * first.astype(jnp.float32) + lowered, norm_second).astype(jnp.bfloat16)
    return lax.map(one_block, blocks).reshape(tokens.shape[0], D)
```

```python
import jax
import jax.numpy as jnp
from jax import lax
from jax.experimental import pallas as pl
from jax.experimental.pallas import tpu as pltpu
from jax.sharding import Mesh
from jax.sharding import PartitionSpec as P

SEQ = 128
FS = ("fs_0", "fs_1", "fs_2")
REP_FS_TP = ("rep", "fs_0", "fs_1", "fs_2", "tp")
MESH = pl.DeviceIdType.MESH
SCALE = 2.0**0.25
EPS = 1e-05
F32 = jnp.float32
BF16 = jnp.bfloat16

D = 2048
ROWS = 64
TOK = 384
CH = 384
HID = 1024
NSEQ = TOK // SEQ
WIDTHS = (3 * CH, CH, HID, HID)
PROJ, MIX, UP, DOWN = range(4)


def kernel(
    tok, pin, min_, uin, din, taps, gain1, gain2, out,
    wp, wm, wu, wd, x, f, mixed, hid, pd, d_send, d_recv, z_send, z_recv, acc,
    sw_send, sw_recv, sw_own, sz_send, sz_recv, sx_own, sx_send, sx_recv, sf_send, sf_recv,
    sd_send, sd_recv, sr_send, sr_recv, s_out,
):
    rep, zl = lax.axis_index("rep"), lax.axis_index("fs_0")
    my_y, my_x, core = lax.axis_index("fs_1"), lax.axis_index("fs_2"), lax.axis_index("tp")
    z = rep * 2 + zl

    def device(z_, y_, x_, c_):
        return (z_ // 2, z_ % 2, y_, x_, c_)

    z_plus, z_minus = (z + 1) % 4, (z + 3) % 4
    above, below = device(z_plus, my_y, my_x, core), device(z_minus, my_y, my_x, core)
    sibling = device(z, my_y, my_x, 1 - core)
    z_to = (z + 3 + 2 * core) % 4
    z_from = (z + 1 + 2 * core) % 4
    helper, helped = device(z_to, my_y, my_x, core), device(z_from, my_y, my_x, core)
    x_plus, x_minus = device(z, my_y, (my_x + 1) % 4, core), device(z, my_y, (my_x + 3) % 4, core)
    y_plus, y_minus = device(z, (my_y + 1) % 4, my_x, core), device(z, (my_y + 3) % 4, my_x, core)

    weights = (wp, wm, wu, wd)
    shards = (pin, min_, uin, din)
    own_row = pl.multiple_of(((zl * 4 + my_y) * 4 + my_x) * ROWS, ROWS)

    def block_row(color, i1, i2):
        y_, x_ = (i2, i1) if color == 0 else (i1, i2)
        return pl.multiple_of(((color * 4 + y_) * 4 + x_) * ROWS, ROWS)

    me = ((my_x, my_y), (my_y, my_x))
    plus = ((x_plus, y_plus), (y_plus, x_plus))
    minus = ((x_minus, y_minus), (y_minus, x_minus))
    SHIFT = (0, 3, 1, 2)

    def block(color, k1, k2):
        return block_row(color, (me[color][0] + SHIFT[k1]) % 4, (me[color][1] + SHIFT[k2]) % 4)

    def wcopy(t, color, slot, row, rows, target):
        part = weights[t].at[pl.ds(row, rows)]
        return pltpu.make_async_remote_copy(
            src_ref=part, dst_ref=part, send_sem=sw_send.at[t], recv_sem=sw_recv.at[t, color, slot],
            device_id=target, device_id_type=MESH,
        )

    HALF = ROWS // 2

    def first_leg(t, color):
        row = block(color, 0, 0)
        wcopy(t, color, 0, row, ROWS, plus[color][0]).start()
        wcopy(t, color, 1, row, ROWS, minus[color][0]).start()

    def second_leg(t, color, k):
        row = block(color, k, 0)
        wcopy(t, color, 4 + 4 * k, row, ROWS, plus[color][1]).start()
        wcopy(t, color, 5 + 4 * k, row, ROWS, minus[color][1]).start()

    def arrive(t, color, slot, row, rows):
        wcopy(t, color, slot, row, rows, plus[color][0]).wait_recv()

    def zcopy(t, half, row, target):
        return pltpu.make_async_remote_copy(
            src_ref=shards[t].at[1 - zl, pl.ds(half * HALF, HALF)],
            dst_ref=weights[t].at[pl.ds(row + half * HALF, HALF)],
            send_sem=sz_send.at[t, half], recv_sem=sz_recv.at[t, half],
            device_id=target, device_id_type=MESH,
        )

    other_row = pl.multiple_of((((1 - zl) * 4 + my_y) * 4 + my_x) * ROWS, ROWS)

    def own_copy(t):
        return pltpu.make_async_copy(shards[t].at[zl], weights[t].at[pl.ds(own_row, ROWS)], sw_own.at[t])

    def start_z(t):
        zcopy(t, 0, own_row, above).start()
        zcopy(t, 1, own_row, below).start()

    def g0(t):
        own_copy(t).wait()
        zcopy(t, 0, other_row, above).wait_recv()
        zcopy(t, 1, other_row, below).wait_recv()
        for color in (0, 1):
            first_leg(t, color)
        for color in (0, 1):
            second_leg(t, color, 0)

    def g1(t):
        for color in (0, 1):
            row = block(color, 1, 0)
            arrive(t, color, 0, row, ROWS)
            wcopy(t, color, 2, row, HALF, plus[color][0]).start()
        for color in (0, 1):
            row = block(color, 2, 0)
            arrive(t, color, 1, row, ROWS)
            wcopy(t, color, 3, row + HALF, HALF, minus[color][0]).start()
        for color in (0, 1):
            second_leg(t, color, 1)
            second_leg(t, color, 2)

    def g2(t):
        for color in (0, 1):
            row = block(color, 3, 0)
            arrive(t, color, 2, row, HALF)
            arrive(t, color, 3, row + HALF, HALF)
            second_leg(t, color, 3)

    def g3(t, k):
        for color in (0, 1):
            row = block(color, k, 1)
            arrive(t, color, 4 + 4 * k, row, ROWS)
            wcopy(t, color, 6 + 4 * k, row, HALF, plus[color][1]).start()
            row = block(color, k, 2)
            arrive(t, color, 5 + 4 * k, row, ROWS)
            wcopy(t, color, 7 + 4 * k, row + HALF, HALF, minus[color][1]).start()

    def g4(t):
        for k in range(4):
            for color in (0, 1):
                row = block(color, k, 3)
                arrive(t, color, 6 + 4 * k, row, HALF)
                arrive(t, color, 7 + 4 * k, row + HALF, HALF)

    def seq(s):
        return pl.ds(s * SEQ, SEQ)

    def tok_z(s):
        return pltpu.make_async_remote_copy(
            src_ref=tok.at[seq(s)], dst_ref=x.at[2, seq(s)], send_sem=sx_send.at[0],
            recv_sem=sx_recv.at[1 + s], device_id=helper, device_id_type=MESH,
        )

    def tok_sibling():
        return pltpu.make_async_remote_copy(
            src_ref=tok, dst_ref=x.at[1], send_sem=sx_send.at[1],
            recv_sem=sx_recv.at[0], device_id=sibling, device_id_type=MESH,
        )

    def tok_relay(s):
        return pltpu.make_async_remote_copy(
            src_ref=x.at[2, seq(s)], dst_ref=x.at[3, seq(s)], send_sem=sx_send.at[2],
            recv_sem=sx_recv.at[4 + s], device_id=sibling, device_id_type=MESH,
        )

    def first_copy(kind, s):
        source, target, to = ((0, 1, sibling), (0, 2, helper), (2, 3, sibling))[kind]
        return pltpu.make_async_remote_copy(
            src_ref=f.at[source, seq(s)], dst_ref=f.at[target, seq(s)], send_sem=sf_send.at[kind],
            recv_sem=sf_recv.at[kind, s], device_id=to, device_id_type=MESH,
        )

    def part_copy(phase, slot, s):
        return pltpu.make_async_remote_copy(
            src_ref=d_send.at[slot, seq(s)], dst_ref=d_recv.at[slot, seq(s)], send_sem=sd_send.at[phase, slot],
            recv_sem=sd_recv.at[phase, slot, s], device_id=sibling, device_id_type=MESH,
        )

    def sum_copy(phase, s):
        return pltpu.make_async_remote_copy(
            src_ref=z_send.at[seq(s)], dst_ref=z_recv.at[seq(s)], send_sem=sr_send.at[phase],
            recv_sem=sr_recv.at[phase, s], device_id=helped, device_id_type=MESH,
        )

    def relay_tokens(s):
        tok_z(s).wait_recv()
        tok_relay(s).start()

    def all_sent(ref, sem):
        pltpu.make_async_remote_copy(
            src_ref=ref, dst_ref=ref, send_sem=sem, recv_sem=sw_recv.at[0, 0, 0], device_id=x_plus, device_id_type=MESH
        ).wait_send()

    row_id = lax.broadcasted_iota(jnp.int32, (SEQ, 1), 0)

    def convolve(g, at, ch, c0):
        for s in range(NSEQ):
            rows = pl.ds(s * SEQ, SEQ)
            product = pd[rows, pl.ds(ch, ch)] * pd[rows, pl.ds(2 * ch, ch)]
            before = jnp.where(row_id > 0, pltpu.roll(product, 1, 0), 0.0)
            after = jnp.where(row_id < SEQ - 1, pltpu.roll(product, SEQ - 1, 0), 0.0)
            conv = taps[0:1, c0:c0 + ch] * before + taps[1:2, c0:c0 + ch] * product + taps[2:3, c0:c0 + ch] * after
            mixed[g, rows, c0:c0 + ch] = (pd[rows, pl.ds(0, ch)] * conv).astype(BF16)

    def project(g):
        pd[...] = jnp.dot(x[g], wp[:, 0:768], preferred_element_type=F32)
        convolve(g, 0, 256, 0)
        pd[:, 0:384] = jnp.dot(x[g], wp[:, 768:1152], preferred_element_type=F32)
        convolve(g, 768, 128, 256)

    def times_transposed(rows_of, w, emit):
        def step(j, _):
            cols = pl.ds(pl.multiple_of(j * 512, 512), 512)
            emit(cols, lax.dot_general(rows_of(), w[cols, :], (((1,), (1,)), ((), ())), preferred_element_type=F32))
            return 0

        lax.fori_loop(0, D // 512, step, 0)

    def partial_sums(phase, source, w, g, s=None):
        rows = pl.ds(0, TOK) if s is None else seq(s)
        parts = range(NSEQ) if s is None else (s,)
        slot = g // 2
        if g in (1, 3):

            def emit(cols, total):
                d_send[slot, rows, cols] = total.astype(BF16)

        else:
            for part in parts:
                part_copy(phase, slot, part).wait_recv()

            def emit(cols, total):
                total = total + d_recv[slot, rows, cols].astype(F32)
                if g == 2:
                    z_send[rows, cols] = total.astype(BF16)
                else:
                    acc[rows, cols] = total

        times_transposed(lambda: source[g, rows, :], w, emit)
        for part in parts:
            if g in (1, 3):
                part_copy(phase, slot, part).start()
            elif g == 2:
                sum_copy(phase, part).start()

    def normed(phase, base, gain, s, target):
        sum_copy(phase, s).wait_recv()
        step_rows = 32

        def step(i, _):
            rows = pl.ds(pl.multiple_of(s * SEQ + i * step_rows, step_rows), step_rows)
            v = SCALE * base[0, rows, :].astype(F32) + (acc[rows, :] + z_recv[rows, :].astype(F32))
            center = v - jnp.mean(v, axis=-1, keepdims=True)
            spread = jnp.mean(center * center, axis=-1, keepdims=True)
            target(rows, (center * lax.rsqrt(spread + EPS) * gain[...]).astype(BF16))
            return 0

        lax.fori_loop(0, SEQ // step_rows, step, 0)

    def to_first(rows, value):
        f[0, rows, :] = value

    def to_result(rows, value):
        z_send[rows, :] = value

    def expand(g):
        def step(j, _):
            cols = pl.ds(pl.multiple_of(j * 512, 512), 512)
            raised = jnp.maximum(jnp.dot(f[g], wu[:, cols], preferred_element_type=F32), 0.0)
            hid[g, :, cols] = (raised * raised).astype(BF16)
            return 0

        lax.fori_loop(0, HID // 512, step, 0)

    barrier = pltpu.get_barrier_semaphore()
    for other in (x_plus, x_minus, y_plus, y_minus, above, below, sibling):
        pl.semaphore_signal(barrier, inc=1, device_id=other, device_id_type=MESH)
    own_tokens = pltpu.make_async_copy(tok, x.at[0], sx_own)
    for t in range(4):
        own_copy(t).start()
    own_tokens.start()
    pl.semaphore_wait(barrier, 7)

    start_z(PROJ)
    start_z(MIX)
    tok_z(0).start()
    start_z(UP)
    tok_z(1).start()
    start_z(DOWN)
    tok_z(2).start()
    tok_sibling().start()

    g0(PROJ)
    g1(PROJ)
    g3(PROJ, 0)
    relay_tokens(0)
    g2(PROJ)
    g3(PROJ, 1)
    relay_tokens(1)
    g3(PROJ, 2)
    g0(MIX)
    relay_tokens(2)
    g3(PROJ, 3)
    g0(UP)
    g1(MIX)
    g3(MIX, 0)
    g4(PROJ)
    for s in range(NSEQ):
        tok_relay(s).wait_recv()
    project(3)
    g2(MIX)
    g3(MIX, 1)
    g3(MIX, 2)
    g1(UP)
    g3(MIX, 3)
    g3(UP, 0)
    project(2)
    g4(MIX)
    for s in range(NSEQ):
        partial_sums(0, mixed, wm, 3, s)
    for s in range(NSEQ):
        partial_sums(0, mixed, wm, 2, s)
    g2(UP)
    g3(UP, 1)
    tok_sibling().wait_recv()
    project(1)
    g3(UP, 2)
    g0(DOWN)
    g3(UP, 3)
    partial_sums(0, mixed, wm, 1)
    own_tokens.wait()
    project(0)
    g1(DOWN)
    g3(DOWN, 0)
    partial_sums(0, mixed, wm, 0)
    g4(UP)
    for s in range(NSEQ):
        normed(0, x, gain1, s, to_first)
        first_copy(1, s).start()
        first_copy(0, s).start()
        if s == 0:
            g2(DOWN)
            g3(DOWN, 1)
        if s == 1:
            g3(DOWN, 2)
            g3(DOWN, 3)
    expand(0)
    for s in range(NSEQ):
        first_copy(0, s).wait_recv()
    expand(1)
    for s in range(NSEQ):
        first_copy(1, s).wait_recv()
        first_copy(2, s).start()
    expand(2)
    for s in range(NSEQ):
        first_copy(2, s).wait_recv()
    expand(3)
    for slot in (0, 1):
        all_sent(d_send.at[slot], sd_send.at[0, slot])
    all_sent(z_send, sr_send.at[0])
    g4(DOWN)
    for s in range(NSEQ):
        partial_sums(1, hid, wd, 3, s)
    for s in range(NSEQ):
        partial_sums(1, hid, wd, 2, s)
    partial_sums(1, hid, wd, 1)
    partial_sums(1, hid, wd, 0)
    all_sent(z_send, sr_send.at[1])
    results = []
    for s in range(NSEQ):
        normed(1, f, gain2, s, to_result)
        results.append(pltpu.make_async_copy(z_send.at[seq(s)], out.at[seq(s)], s_out.at[s]))
        results[-1].start()

    for t in range(4):
        all_sent(weights[t].at[pl.ds(0, 30 * ROWS)], sw_send.at[t])
        zcopy(t, 0, own_row, above).wait_send()
        zcopy(t, 1, own_row, below).wait_send()
    for kind in range(3):
        all_sent(x.at[0], sx_send.at[kind])
        all_sent(f.at[0], sf_send.at[kind])
    for slot in (0, 1):
        all_sent(d_send.at[slot], sd_send.at[1, slot])
    for result in results:
        result.wait()


def local(tokens, outer_weight, inner_weight, value_weight, conv_taps, mix_out, norm_first, up_weight, down_weight, norm_second):
    o, i, v = (w.astype(BF16) for w in (outer_weight, inner_weight, value_weight))
    halves = []
    for h in (0, 1):
        a, b, c = h * CH, h * CH + 256, (h + 1) * CH
        halves.append(jnp.concatenate([w[:, a:b] for w in (o, i, v)] + [w[:, b:c] for w in (o, i, v)], axis=1))
    pin = jnp.stack(halves)

    def split(w, width):
        return w.astype(BF16).reshape(ROWS, 2, width).transpose(1, 0, 2)

    min_ = split(mix_out.T, CH)
    uin = split(up_weight, HID)
    din = split(down_weight.T, HID)
    zl = lax.axis_index("fs_0")
    taps = lax.dynamic_slice_in_dim(conv_taps, zl * CH, CH, axis=1)

    hbm = pl.BlockSpec(memory_space=pl.ANY)
    vmem = pl.BlockSpec(memory_space=pltpu.VMEM)
    dma = pltpu.SemaphoreType.DMA
    return pl.pallas_call(
        kernel,
        name="mixer_ffn",
        out_shape=jax.ShapeDtypeStruct((TOK, D), BF16),
        in_specs=[hbm] * 5 + [vmem] * 3,
        out_specs=hbm,
        scratch_shapes=[pltpu.VMEM((D, w), BF16) for w in WIDTHS]
        + [
            pltpu.VMEM((4, TOK, D), BF16),
            pltpu.VMEM((4, TOK, D), BF16),
            pltpu.VMEM((4, TOK, CH), BF16),
            pltpu.VMEM((4, TOK, HID), BF16),
            pltpu.VMEM((TOK, 768), F32),
            pltpu.VMEM((2, TOK, D), BF16),
            pltpu.VMEM((2, TOK, D), BF16),
            pltpu.VMEM((TOK, D), BF16),
            pltpu.VMEM((TOK, D), BF16),
            pltpu.VMEM((TOK, D), F32),
            dma((4,)),
            dma((4, 2, 20)),
            dma((4,)),
            dma((4, 2)),
            dma((4, 2)),
            dma,
            dma((3,)),
            dma((7,)),
            dma((3,)),
            dma((3, 3)),
            dma((2, 2)),
            dma((2, 2, 3)),
            dma((2,)),
            dma((2, 3)),
            dma((3,)),
        ],
        compiler_params=pltpu.CompilerParams(
            collective_id=0, has_side_effects=True, vmem_limit_bytes=62 * 1024 * 1024
        ),
    )(tokens, pin, min_, uin, din, taps, norm_first.reshape(1, D), norm_second.reshape(1, D))


def solution(mesh):
    finer = Mesh(
        mesh.devices.reshape(mesh.shape["rep"], 2, 4, 4, mesh.shape["tp"]),
        ("rep", "fs_0", "fs_1", "fs_2", "tp"),
    )
    placed = (
        P(REP_FS_TP, None),
        P(FS, "tp"),
        P(FS, "tp"),
        P(FS, "tp"),
        P(None, "tp"),
        P("tp", FS),
        P(),
        P(FS, "tp"),
        P("tp", FS),
        P(),
    )
    return jax.shard_map(
        local, mesh=finer, in_specs=placed, out_specs=P(REP_FS_TP, None), check_vma=False
    )
```

```python
import jax
import jax.numpy as jnp
from jax import lax
from jax.experimental import pallas as pl
from jax.experimental.pallas import tpu as pltpu
from jax.sharding import Mesh
from jax.sharding import PartitionSpec as P

SEQ = 128
FS = ("fs_0", "fs_1", "fs_2")
REP_FS_TP = ("rep", "fs_0", "fs_1", "fs_2", "tp")
MESH = pl.DeviceIdType.MESH
SCALE = 2.0**0.25
EPS = 1e-05
F32 = jnp.float32
BF16 = jnp.bfloat16

D = 2048
ROWS = 64
TOK = 384
CH = 384
HID = 1024
NSEQ = TOK // SEQ
WIDTHS = (CH, 3 * CH, HID, HID)
MIX, PROJ, UP, DOWN = range(4)
COLS = 512
NCOL = D // COLS


def kernel(
    tok, wo_in, wi_in, wv_in, wm_in, wu_in, wd_in, taps, gain1, gain2, out,
    wm, wp, wu, wd, wm2, gm, gp, gu, gd, stage_p, stage_m, stage_u, stage_d,
    x, f, mixed, mixed2, hid, pd, d_send, d_recv, z_send, z_recv, acc,
    s_in, sw_send, sw_recv, sz_send, sz_recv, sx_own, sx_send, sx_recv, sf_send, sf_recv,
    sq_send, sq_recv, sm_send, sm_recv, sd_send, sd_recv, sr_send, sr_recv, s_out,
):
    rep, zl = lax.axis_index("rep"), lax.axis_index("fs_0")
    my_y, my_x, core = lax.axis_index("fs_1"), lax.axis_index("fs_2"), lax.axis_index("tp")
    z = rep * 2 + zl

    def device(z_, y_, x_, c_):
        return (z_ // 2, z_ % 2, y_, x_, c_)

    z_plus, z_minus = (z + 1) % 4, (z + 3) % 4
    above, below = device(z_plus, my_y, my_x, core), device(z_minus, my_y, my_x, core)
    sibling = device(z, my_y, my_x, 1 - core)
    z_to = (z + 3 + 2 * core) % 4
    z_from = (z + 1 + 2 * core) % 4
    helper, helped = device(z_to, my_y, my_x, core), device(z_from, my_y, my_x, core)
    x_plus, x_minus = device(z, my_y, (my_x + 1) % 4, core), device(z, my_y, (my_x + 3) % 4, core)
    y_plus, y_minus = device(z, (my_y + 1) % 4, my_x, core), device(z, (my_y + 3) % 4, my_x, core)

    def remote(src, dst, send_sem, recv_sem, target):
        return pltpu.make_async_remote_copy(
            src_ref=src, dst_ref=dst, send_sem=send_sem, recv_sem=recv_sem, device_id=target, device_id_type=MESH
        )

    weights = (wm, wp, wu, wd)
    given = (gm, gp, gu, gd)
    own_row = pl.multiple_of(((zl * 4 + my_y) * 4 + my_x) * ROWS, ROWS)
    other_row = pl.multiple_of((((1 - zl) * 4 + my_y) * 4 + my_x) * ROWS, ROWS)

    def load(which):
        pairs = (
            (wm_in, stage_m), (wo_in, stage_p.at[0]), (wi_in, stage_p.at[1]), (wv_in, stage_p.at[2]),
            (wu_in, stage_u), (wd_in, stage_d),
        )
        return pltpu.make_async_copy(*pairs[which], s_in.at[which])

    def cast(t):
        keep, give = weights[t], given[t]
        rows = pl.ds(own_row, ROWS)
        if t == PROJ:
            for which in (1, 2, 3):
                load(which).wait()
            for width, c0, at in ((256, 0, 0), (128, 256, 768)):
                for i in range(3):
                    mine = pl.ds(pl.multiple_of(zl * CH + c0, 128), width)
                    theirs = pl.ds(pl.multiple_of((1 - zl) * CH + c0, 128), width)
                    cols = slice(at + i * width, at + (i + 1) * width)
                    keep[rows, cols] = stage_p[i, :, mine].astype(BF16)
                    give[:, cols] = stage_p[i, :, theirs].astype(BF16)
        else:
            stage = {MIX: stage_m, UP: stage_u, DOWN: stage_d}[t]
            load({MIX: 0, UP: 4, DOWN: 5}[t]).wait()
            width = WIDTHS[t]
            keep[rows, :] = stage[:, pl.ds(pl.multiple_of(zl * width, 128), width)].astype(BF16)
            give[...] = stage[:, pl.ds(pl.multiple_of((1 - zl) * width, 128), width)].astype(BF16)

    me = ((my_x, my_y), (my_y, my_x))
    plus = ((x_plus, y_plus), (y_plus, x_plus))
    minus = ((x_minus, y_minus), (y_minus, x_minus))
    SHIFT = (0, 3, 1, 2)
    HALF = ROWS // 2

    def block(color, k1, k2):
        i1, i2 = (me[color][0] + SHIFT[k1]) % 4, (me[color][1] + SHIFT[k2]) % 4
        y_, x_ = (i2, i1) if color == 0 else (i1, i2)
        return pl.multiple_of(((color * 4 + y_) * 4 + x_) * ROWS, ROWS)

    def wcopy(t, color, slot, row, rows, target):
        part = weights[t].at[pl.ds(row, rows)]
        return remote(part, part, sw_send.at[t], sw_recv.at[t, color, slot], target)

    def second_leg(t, color, k):
        row = block(color, k, 0)
        wcopy(t, color, 4 + 4 * k, row, ROWS, plus[color][1]).start()
        wcopy(t, color, 5 + 4 * k, row, ROWS, minus[color][1]).start()

    def arrive(t, color, slot, row, rows):
        wcopy(t, color, slot, row, rows, plus[color][0]).wait_recv()

    def zcopy(t, half, row, target):
        return remote(
            given[t].at[pl.ds(half * HALF, HALF)], weights[t].at[pl.ds(row + half * HALF, HALF)],
            sz_send.at[t, half], sz_recv.at[t, half], target,
        )

    def start_z(t):
        zcopy(t, 0, own_row, above).start()
        zcopy(t, 1, own_row, below).start()

    def both_legs(t, color, row):
        for slot, step in ((0, 1), (1, 3)):
            wcopy(t, color, slot, row, ROWS, device(z, (my_y + step * color) % 4, (my_x + step * (1 - color)) % 4, core)).start()
        for slot, step in ((4, 1), (5, 3)):
            wcopy(t, color, slot, row, ROWS, device(z, (my_y + step * (1 - color)) % 4, (my_x + step * color) % 4, core)).start()

    def g0_own(t):
        both_legs(t, zl, own_row)

    def g0_other(t):
        zcopy(t, 0, other_row, above).wait_recv()
        zcopy(t, 1, other_row, below).wait_recv()
        both_legs(t, 1 - zl, other_row)

    def g1(t):
        for color in (0, 1):
            row = block(color, 1, 0)
            arrive(t, color, 0, row, ROWS)
            wcopy(t, color, 2, row, HALF, plus[color][0]).start()
        for color in (0, 1):
            row = block(color, 2, 0)
            arrive(t, color, 1, row, ROWS)
            wcopy(t, color, 3, row + HALF, HALF, minus[color][0]).start()
        for color in (0, 1):
            second_leg(t, color, 1)
            second_leg(t, color, 2)

    def g2(t):
        for color in (0, 1):
            row = block(color, 3, 0)
            arrive(t, color, 2, row, HALF)
            arrive(t, color, 3, row + HALF, HALF)
            second_leg(t, color, 3)

    def g3(t, k):
        for color in (0, 1):
            row = block(color, k, 1)
            arrive(t, color, 4 + 4 * k, row, ROWS)
            wcopy(t, color, 6 + 4 * k, row, HALF, plus[color][1]).start()
            row = block(color, k, 2)
            arrive(t, color, 5 + 4 * k, row, ROWS)
            wcopy(t, color, 7 + 4 * k, row + HALF, HALF, minus[color][1]).start()

    def g4(t):
        for k in range(4):
            for color in (0, 1):
                row = block(color, k, 3)
                arrive(t, color, 6 + 4 * k, row, HALF)
                arrive(t, color, 7 + 4 * k, row + HALF, HALF)

    def mix_swap(color):
        rows = pl.ds(color * 1024, 1024)
        return remote(wm.at[rows], wm2.at[rows], sq_send.at[color], sq_recv.at[color], (above, below)[color])

    def seq(s):
        return pl.ds(s * SEQ, SEQ)

    def tok_z(s):
        return remote(tok.at[seq(s)], x.at[2, seq(s)], sx_send.at[0], sx_recv.at[1 + s], helper)

    def tok_sibling():
        return remote(tok, x.at[1], sx_send.at[1], sx_recv.at[0], sibling)

    def tok_relay(s):
        return remote(x.at[2, seq(s)], x.at[3, seq(s)], sx_send.at[2], sx_recv.at[4 + s], sibling)

    def first_copy(kind, s):
        source, target, to = ((0, 1, sibling), (0, 2, helper), (2, 3, sibling))[kind]
        return remote(f.at[source, seq(s)], f.at[target, seq(s)], sf_send.at[kind], sf_recv.at[kind, s], to)

    def mixed_copy(i):
        return remote(mixed.at[2 + i], mixed2.at[i], sm_send.at[i], sm_recv.at[i], (helped, helper)[i])

    def part_copy(phase, slot, j):
        return remote(d_send.at[slot, j], d_recv.at[slot, j], sd_send.at[phase, slot], sd_recv.at[phase, slot, j], sibling)

    def sum_copy(j):
        return remote(z_send.at[j], z_recv.at[j], sr_send, sr_recv.at[j], helped)

    def relay_tokens(s):
        tok_z(s).wait_recv()
        tok_relay(s).start()

    def all_sent(ref, sem):
        remote(ref, ref, sem, sw_recv.at[0, 0, 0], x_plus).wait_send()

    row_id = lax.broadcasted_iota(jnp.int32, (SEQ, 1), 0)

    def convolve(g, ch, c0):
        tap = [taps[k:k + 1, pl.ds(pl.multiple_of(zl * CH + c0, 128), ch)] for k in range(3)]
        for s in range(NSEQ):
            rows = pl.ds(s * SEQ, SEQ)
            product = pd[rows, pl.ds(ch, ch)] * pd[rows, pl.ds(2 * ch, ch)]
            before = jnp.where(row_id > 0, pltpu.roll(product, 1, 0), 0.0)
            after = jnp.where(row_id < SEQ - 1, pltpu.roll(product, SEQ - 1, 0), 0.0)
            conv = tap[0] * before + tap[1] * product + tap[2] * after
            mixed[g, rows, c0:c0 + ch] = (pd[rows, pl.ds(0, ch)] * conv).astype(BF16)

    def project(g):
        pd[...] = jnp.dot(x[g], wp[:, 0:768], preferred_element_type=F32)
        convolve(g, 256, 0)
        pd[:, 0:384] = jnp.dot(x[g], wp[:, 768:1152], preferred_element_type=F32)
        convolve(g, 128, 256)

    def dot_t(rows, w, j):
        return lax.dot_general(
            rows, w[j * COLS:(j + 1) * COLS, :], (((1,), (1,)), ((), ())), preferred_element_type=F32
        )

    def mix_sums(g):
        for j in range(NCOL):
            total = dot_t(mixed[g], wm, j) + dot_t(mixed2[g], wm2, j)
            if g == 1:
                d_send[0, j] = total.astype(BF16)
                part_copy(0, 0, j).start()
            else:
                acc[:, j * COLS:(j + 1) * COLS] = total

    def ffn_sums(g, j):
        total = dot_t(hid[g], wd, j)
        slot = g // 2
        if g in (1, 3):
            d_send[slot, j] = total.astype(BF16)
            part_copy(1, slot, j).start()
        else:
            part_copy(1, slot, j).wait_recv()
            total = total + d_recv[slot, j].astype(F32)
            if g == 2:
                z_send[j] = total.astype(BF16)
                sum_copy(j).start()
            else:
                acc[:, j * COLS:(j + 1) * COLS] = total

    def normed(base, arrived, gain, s, target):
        step_rows = 32

        def step(i, _):
            rows = pl.ds(pl.multiple_of(s * SEQ + i * step_rows, step_rows), step_rows)
            came = jnp.concatenate([arrived(j, rows) for j in range(NCOL)], axis=1)
            v = SCALE * base[0, rows, :].astype(F32) + (acc[rows, :] + came)
            center = v - jnp.mean(v, axis=-1, keepdims=True)
            spread = jnp.mean(center * center, axis=-1, keepdims=True)
            target[0, rows, :] = (center * lax.rsqrt(spread + EPS) * gain[...]).astype(BF16)
            return 0

        lax.fori_loop(0, SEQ // step_rows, step, 0)

    def expand(g, s=None):
        rows = pl.ds(0, TOK) if s is None else seq(s)

        def step(j, _):
            cols = pl.ds(pl.multiple_of(j * 512, 512), 512)
            raised = jnp.maximum(jnp.dot(f[g, rows, :], wu[:, cols], preferred_element_type=F32), 0.0)
            hid[g, rows, cols] = (raised * raised).astype(BF16)
            return 0

        lax.fori_loop(0, HID // 512, step, 0)

    barrier = pltpu.get_barrier_semaphore()
    for other in (x_plus, x_minus, y_plus, y_minus, above, below, sibling):
        pl.semaphore_signal(barrier, inc=1, device_id=other, device_id_type=MESH)
    own_tokens = pltpu.make_async_copy(tok, x.at[0], sx_own)
    for which in range(6):
        load(which).start()
    own_tokens.start()
    for t in range(4):
        cast(t)
    pl.semaphore_wait(barrier, 7)

    start_z(MIX)
    start_z(PROJ)
    g0_own(MIX)
    g0_own(PROJ)
    tok_z(0).start()
    tok_sibling().start()
    start_z(UP)
    tok_z(1).start()
    tok_z(2).start()
    start_z(DOWN)
    g0_other(MIX)
    g0_other(PROJ)
    g1(MIX)
    g3(MIX, 0)
    g2(MIX)
    g1(PROJ)
    g3(MIX, 1)
    g3(MIX, 2)
    g3(MIX, 3)
    g3(PROJ, 0)
    relay_tokens(0)
    g4(MIX)
    mix_swap(0).start()
    mix_swap(1).start()
    g2(PROJ)
    g3(PROJ, 1)
    relay_tokens(1)
    g3(PROJ, 2)
    relay_tokens(2)
    g3(PROJ, 3)
    g0_own(UP)
    g0_other(UP)
    for s in range(NSEQ):
        tok_relay(s).wait_recv()
    g4(PROJ)
    project(3)
    mixed_copy(1).start()
    g1(UP)
    g3(UP, 0)
    project(2)
    mixed_copy(0).start()
    tok_sibling().wait_recv()
    g2(UP)
    g3(UP, 1)
    project(1)
    g3(UP, 2)
    mix_swap(0).wait_recv()
    mix_swap(1).wait_recv()
    mixed_copy(1).wait_recv()
    mix_sums(1)
    g3(UP, 3)
    g0_own(DOWN)
    g0_other(DOWN)
    own_tokens.wait()
    project(0)
    mixed_copy(0).wait_recv()
    mix_sums(0)
    for j in range(NCOL):
        part_copy(0, 0, j).wait_recv()
    for s in range(NSEQ):
        normed(x, lambda j, rows: d_recv[0, j, rows, :].astype(F32), gain1, s, f)
        first_copy(1, s).start()
        first_copy(0, s).start()
    g4(UP)
    g1(DOWN)
    g3(DOWN, 0)
    expand(0)
    g2(DOWN)
    g3(DOWN, 1)
    for s in range(NSEQ):
        first_copy(0, s).wait_recv()
    expand(1)
    g3(DOWN, 2)
    all_sent(d_send.at[0], sd_send.at[0, 0])
    for s in range(NSEQ):
        first_copy(1, s).wait_recv()
        first_copy(2, s).start()
        expand(2, s)
        if s == 0:
            g3(DOWN, 3)
        first_copy(2, s).wait_recv()
        expand(3, s)
    g4(DOWN)
    ffn_sums(3, 0)
    ffn_sums(3, 1)
    ffn_sums(2, 0)
    ffn_sums(3, 2)
    ffn_sums(2, 1)
    ffn_sums(3, 3)
    ffn_sums(2, 2)
    ffn_sums(2, 3)
    for j in range(NCOL):
        ffn_sums(1, j)
    for j in range(NCOL):
        ffn_sums(0, j)
    for j in range(NCOL):
        sum_copy(j).wait_recv()
    results = []
    for s in range(NSEQ):
        normed(f, lambda j, rows: z_recv[j, rows, :].astype(F32), gain2, s, x)
        results.append(pltpu.make_async_copy(x.at[0, seq(s)], out.at[seq(s)], s_out.at[s]))
        results[-1].start()

    for t in range(4):
        all_sent(weights[t].at[pl.ds(0, 30 * ROWS)], sw_send.at[t])
        zcopy(t, 0, own_row, above).wait_send()
        zcopy(t, 1, own_row, below).wait_send()
    for kind in range(3):
        all_sent(x.at[0], sx_send.at[kind])
        all_sent(f.at[0], sf_send.at[kind])
    for i in (0, 1):
        mix_swap(i).wait_send()
        mixed_copy(i).wait_send()
        all_sent(d_send.at[i], sd_send.at[1, i])
    all_sent(z_send, sr_send)
    for result in results:
        result.wait()


def local(tokens, outer_weight, inner_weight, value_weight, conv_taps, mix_out, norm_first, up_weight, down_weight, norm_second):
    hbm = pl.BlockSpec(memory_space=pl.ANY)
    vmem = pl.BlockSpec(memory_space=pltpu.VMEM)
    dma = pltpu.SemaphoreType.DMA
    return pl.pallas_call(
        kernel,
        name="mixer_ffn",
        out_shape=jax.ShapeDtypeStruct((TOK, D), BF16),
        in_specs=[hbm] * 7 + [vmem] * 3,
        out_specs=hbm,
        scratch_shapes=[pltpu.VMEM((D, w), BF16) for w in WIDTHS]
        + [pltpu.VMEM((D, CH), BF16)]
        + [pltpu.VMEM((ROWS, w), BF16) for w in WIDTHS]
        + [
            pltpu.VMEM((3, ROWS, 2 * CH), F32),
            pltpu.VMEM((ROWS, 2 * CH), F32),
            pltpu.VMEM((ROWS, 2 * HID), F32),
            pltpu.VMEM((ROWS, 2 * HID), F32),
            pltpu.VMEM((4, TOK, D), BF16),
            pltpu.VMEM((4, TOK, D), BF16),
            pltpu.VMEM((4, TOK, CH), BF16),
            pltpu.VMEM((2, TOK, CH), BF16),
            pltpu.VMEM((4, TOK, HID), BF16),
            pltpu.VMEM((TOK, 768), F32),
            pltpu.VMEM((2, NCOL, TOK, COLS), BF16),
            pltpu.VMEM((2, NCOL, TOK, COLS), BF16),
            pltpu.VMEM((NCOL, TOK, COLS), BF16),
            pltpu.VMEM((NCOL, TOK, COLS), BF16),
            pltpu.VMEM((TOK, D), F32),
            dma((6,)),
            dma((4,)),
            dma((4, 2, 20)),
            dma((4, 2)),
            dma((4, 2)),
            dma,
            dma((3,)),
            dma((7,)),
            dma((3,)),
            dma((3, 3)),
            dma((2,)),
            dma((2,)),
            dma((2,)),
            dma((2,)),
            dma((2, 2)),
            dma((2, 2, 4)),
            dma,
            dma((4,)),
            dma((3,)),
        ],
        compiler_params=pltpu.CompilerParams(
            collective_id=0, has_side_effects=True, vmem_limit_bytes=62 * 1024 * 1024
        ),
    )(
        tokens, outer_weight, inner_weight, value_weight, mix_out.T, up_weight, down_weight.T,
        conv_taps, norm_first.reshape(1, D), norm_second.reshape(1, D),
    )


def solution(mesh):
    finer = Mesh(
        mesh.devices.reshape(mesh.shape["rep"], 2, 4, 4, mesh.shape["tp"]),
        ("rep", "fs_0", "fs_1", "fs_2", "tp"),
    )
    placed = (
        P(REP_FS_TP, None),
        P(FS, "tp"),
        P(FS, "tp"),
        P(FS, "tp"),
        P(None, "tp"),
        P("tp", FS),
        P(),
        P(FS, "tp"),
        P("tp", FS),
        P(),
    )
    return jax.shard_map(
        local, mesh=finer, in_specs=placed, out_specs=P(REP_FS_TP, None), check_vma=False
    )
```

```python
import jax
import jax.numpy as jnp
from jax import lax
from jax.experimental import pallas as pl
from jax.experimental.pallas import tpu as pltpu
from jax.sharding import Mesh
from jax.sharding import PartitionSpec as P

SEQ = 128
FS = ("fs_0", "fs_1", "fs_2")
REP_FS_TP = ("rep", "fs_0", "fs_1", "fs_2", "tp")
MESH = pl.DeviceIdType.MESH
SCALE = 2.0**0.25
EPS = 1e-05
F32 = jnp.float32
BF16 = jnp.bfloat16

D = 2048
ROWS = 64
TOK = 384
CH = 384
HID = 1024
NSEQ = TOK // SEQ
WIDTHS = (4 * CH, HID, HID)
MIXER, UP, DOWN = range(3)
COLS = 256
NCOL = D // COLS


def kernel(
    tok, wo_in, wi_in, wv_in, wm_in, wu_in, wd_in, taps, gain1, gain2, out,
    wp, wu, wd, wm2, gp, gu, gd, stage_p, stage_u, stage_d,
    x, f, mixed, mixed2, hid, pd, d_send, d_recv, z_send, z_recv, acc, held,
    s_in, sw_send, sw_recv, sz_send, sz_recv, sx_own, sx_send, sx_recv, sf_send, sf_recv,
    sq_send, sq_recv, sm_send, sm_recv, sd_send, sd_recv, sr_send, sr_recv, s_out,
):
    rep, zl = lax.axis_index("rep"), lax.axis_index("fs_0")
    my_y, my_x, core = lax.axis_index("fs_1"), lax.axis_index("fs_2"), lax.axis_index("tp")
    z = rep * 2 + zl

    def device(z_, y_, x_, c_):
        return (z_ // 2, z_ % 2, y_, x_, c_)

    z_plus, z_minus = (z + 1) % 4, (z + 3) % 4
    above, below = device(z_plus, my_y, my_x, core), device(z_minus, my_y, my_x, core)
    sibling = device(z, my_y, my_x, 1 - core)
    z_to = (z + 3 + 2 * core) % 4
    z_from = (z + 1 + 2 * core) % 4
    helper, helped = device(z_to, my_y, my_x, core), device(z_from, my_y, my_x, core)
    x_plus, x_minus = device(z, my_y, (my_x + 1) % 4, core), device(z, my_y, (my_x + 3) % 4, core)
    y_plus, y_minus = device(z, (my_y + 1) % 4, my_x, core), device(z, (my_y + 3) % 4, my_x, core)

    def remote(src, dst, send_sem, recv_sem, target):
        return pltpu.make_async_remote_copy(
            src_ref=src, dst_ref=dst, send_sem=send_sem, recv_sem=recv_sem, device_id=target, device_id_type=MESH
        )

    weights = (wp, wu, wd)
    given = (gp, gu, gd)
    own_row = (zl * 4 + my_y, my_x)
    other_row = ((1 - zl) * 4 + my_y, my_x)

    def load(which):
        pairs = (
            (wo_in, stage_p.at[0]), (wi_in, stage_p.at[1]), (wv_in, stage_p.at[2]), (wm_in, stage_p.at[3]),
            (wu_in, stage_u), (wd_in, stage_d),
        )
        return pltpu.make_async_copy(*pairs[which], s_in.at[which])

    def cast(t):
        keep, give = weights[t].at[own_row[0], own_row[1]], given[t]
        if t == MIXER:
            for which in range(4):
                load(which).wait()
            pieces = [(i, c0, at + i * width, width) for width, c0, at in ((256, 0, 0), (128, 256, 768)) for i in range(3)]
            for i, c0, at, width in pieces + [(3, 0, 3 * CH, CH)]:
                mine = pl.ds(pl.multiple_of(zl * CH + c0, 128), width)
                theirs = pl.ds(pl.multiple_of((1 - zl) * CH + c0, 128), width)
                keep[:, at:at + width] = stage_p[i, :, mine].astype(BF16)
                give[:, at:at + width] = stage_p[i, :, theirs].astype(BF16)
        else:
            stage = {UP: stage_u, DOWN: stage_d}[t]
            load({UP: 4, DOWN: 5}[t]).wait()
            width = WIDTHS[t]
            keep[...] = stage[:, pl.ds(pl.multiple_of(zl * width, 128), width)].astype(BF16)
            give[...] = stage[:, pl.ds(pl.multiple_of((1 - zl) * width, 128), width)].astype(BF16)

    me = ((my_x, my_y), (my_y, my_x))
    plus = ((x_plus, y_plus), (y_plus, x_plus))
    minus = ((x_minus, y_minus), (y_minus, x_minus))
    SHIFT = (0, 3, 1, 2)
    HALF = ROWS // 2

    def block(color, k1, k2):
        i1, i2 = (me[color][0] + SHIFT[k1]) % 4, (me[color][1] + SHIFT[k2]) % 4
        y_, x_ = (i2, i1) if color == 0 else (i1, i2)
        return (color * 4 + y_, x_)

    def wcopy(t, color, slot, row, start, rows, target):
        part = weights[t].at[row[0], row[1], pl.ds(start, rows)]
        return remote(part, part, sw_send.at[t, int(slot == 0)], sw_recv.at[t, color, slot], target)

    def second_leg(t, color, k):
        row = block(color, k, 0)
        wcopy(t, color, 4 + 4 * k, row, 0, ROWS, plus[color][1]).start()
        wcopy(t, color, 5 + 4 * k, row, 0, ROWS, minus[color][1]).start()

    def arrive(t, color, slot, row, start, rows):
        wcopy(t, color, slot, row, start, rows, plus[color][0]).wait_recv()

    def zcopy(t, half, row, target):
        return remote(
            given[t].at[pl.ds(half * HALF, HALF)], weights[t].at[row[0], row[1], pl.ds(half * HALF, HALF)],
            sz_send.at[t, half], sz_recv.at[t, half], target,
        )

    def start_z(t):
        zcopy(t, 0, own_row, above).start()
        zcopy(t, 1, own_row, below).start()

    def both_legs(t, color, row):
        for slot, step in ((0, 1), (1, 3)):
            wcopy(t, color, slot, row, 0, ROWS, device(z, (my_y + step * color) % 4, (my_x + step * (1 - color)) % 4, core)).start()
        for slot, step in ((4, 1), (5, 3)):
            wcopy(t, color, slot, row, 0, ROWS, device(z, (my_y + step * (1 - color)) % 4, (my_x + step * color) % 4, core)).start()

    def g0_own(t):
        both_legs(t, zl, own_row)

    def g0_other(t):
        zcopy(t, 0, other_row, above).wait_recv()
        zcopy(t, 1, other_row, below).wait_recv()
        both_legs(t, 1 - zl, other_row)

    def g1(t):
        for color in (0, 1):
            row = block(color, 1, 0)
            arrive(t, color, 0, row, 0, ROWS)
            wcopy(t, color, 2, row, 0, HALF, plus[color][0]).start()
        for color in (0, 1):
            row = block(color, 2, 0)
            arrive(t, color, 1, row, 0, ROWS)
            wcopy(t, color, 3, row, HALF, HALF, minus[color][0]).start()
        for color in (0, 1):
            second_leg(t, color, 1)
            second_leg(t, color, 2)

    def g2(t):
        for color in (0, 1):
            row = block(color, 3, 0)
            arrive(t, color, 2, row, 0, HALF)
            arrive(t, color, 3, row, HALF, HALF)
            second_leg(t, color, 3)

    def g3(t, k):
        for color in (0, 1):
            row = block(color, k, 1)
            arrive(t, color, 4 + 4 * k, row, 0, ROWS)
            wcopy(t, color, 6 + 4 * k, row, 0, HALF, plus[color][1]).start()
            row = block(color, k, 2)
            arrive(t, color, 5 + 4 * k, row, 0, ROWS)
            wcopy(t, color, 7 + 4 * k, row, HALF, HALF, minus[color][1]).start()

    def g4(t):
        for k in range(4):
            for color in (0, 1):
                row = block(color, k, 3)
                arrive(t, color, 6 + 4 * k, row, 0, HALF)
                arrive(t, color, 7 + 4 * k, row, HALF, HALF)

    def chunk(color, k):
        return (me[color][1] + SHIFT[k]) % 4

    def chunk_rows(ref, color, at):
        return ref.at[at] if color == 0 else ref.at[pl.ds(4, 4), at]

    def mix_swap(k, color):
        source = chunk_rows(wp, color, chunk(color, k)).at[:, :, pl.ds(3 * CH, CH)]
        return remote(
            source, chunk_rows(wm2, color, chunk(color, k)), sq_send.at[k, color], sq_recv.at[k, color], (above, below)[color]
        )

    def seq(s):
        return pl.ds(s * SEQ, SEQ)

    def tok_z(s):
        return remote(tok.at[seq(s)], x.at[2, seq(s)], sx_send.at[0], sx_recv.at[1 + s], helper)

    def tok_sibling():
        return remote(tok, x.at[1], sx_send.at[1], sx_recv.at[0], sibling)

    def tok_relay(s):
        return remote(x.at[2, seq(s)], x.at[3, seq(s)], sx_send.at[2], sx_recv.at[4 + s], sibling)

    def first_copy(kind, s):
        source, target, to = ((0, 1, sibling), (0, 2, helper), (2, 3, sibling))[kind]
        return remote(f.at[source, seq(s)], f.at[target, seq(s)], sf_send.at[kind], sf_recv.at[kind, s], to)

    def mixed_copy(i):
        return remote(mixed.at[2 + i], mixed2.at[i], sm_send.at[i], sm_recv.at[i], (helped, helper)[i])

    def part_copy(phase, slot, i, j):
        return remote(d_send.at[slot, j], d_recv.at[slot, j], sd_send.at[phase, slot], sd_recv.at[phase, slot, i], sibling)

    def sum_copy(k, color):
        j = color * 4 + chunk(color, k)
        return remote(z_send.at[j], z_recv.at[j], sr_send, sr_recv.at[k * 2 + color], helped)

    def relay_tokens(s):
        tok_z(s).wait_recv()
        tok_relay(s).start()

    def all_sent(ref, sem):
        remote(ref, ref, sem, sw_recv.at[0, 0, 0], x_plus).wait_send()

    row_id = lax.broadcasted_iota(jnp.int32, (SEQ, 1), 0)

    def convolve(g, ch, c0):
        tap = [taps[k:k + 1, pl.ds(pl.multiple_of(zl * CH + c0, 128), ch)] for k in range(3)]
        for s in range(NSEQ):
            rows = pl.ds(s * SEQ, SEQ)
            product = pd[rows, pl.ds(ch, ch)] * pd[rows, pl.ds(2 * ch, ch)]
            before = jnp.where(row_id > 0, pltpu.roll(product, 1, 0), 0.0)
            after = jnp.where(row_id < SEQ - 1, pltpu.roll(product, SEQ - 1, 0), 0.0)
            conv = tap[0] * before + tap[1] * product + tap[2] * after
            mixed[g, rows, c0:c0 + ch] = (pd[rows, pl.ds(0, ch)] * conv).astype(BF16)

    def project(g):
        pd[...] = jnp.dot(x[g], wp[:, :, :, 0:768].reshape(D, 768), preferred_element_type=F32)
        convolve(g, 256, 0)
        pd[:, 0:384] = jnp.dot(x[g], wp[:, :, :, 768:1152].reshape(D, 384), preferred_element_type=F32)
        convolve(g, 128, 256)

    def dot_t(rows, w):
        return lax.dot_general(
            rows, w.reshape(COLS, w.shape[-1]), (((1,), (1,)), ((), ())), preferred_element_type=F32
        )

    def pair(ref, g):
        return ref[g:g + 2].reshape(2 * TOK, ref.shape[-1])

    def mix_sums(j):
        total = dot_t(pair(mixed, 0), wp[j, :, :, 3 * CH:4 * CH]) + dot_t(pair(mixed2, 0), wm2[j])
        acc[j] = total[:TOK]
        d_send[0, j] = total[TOK:].astype(BF16)
        part_copy(0, 0, j, j).start()

    def ffn_sums(g, k, color):
        j = color * 4 + chunk(color, k)
        slot = g // 2
        w = wd[j] if color == 0 else wd[4:8, j - 4]
        total = dot_t(pair(hid, g), w)
        d_send[slot, j] = total[TOK:].astype(BF16)
        part_copy(1, slot, k * 2 + color, j).start()
        if g == 0:
            acc[j] = total[:TOK]
        else:
            held[k % 2, color] = total[:TOK]

    def ffn_send(k, color):
        j = color * 4 + chunk(color, k)
        part_copy(1, 1, k * 2 + color, j).wait_recv()
        z_send[j] = (held[k % 2, color] + d_recv[1, j].astype(F32)).astype(BF16)
        sum_copy(k, color).start()

    low = lax.broadcasted_iota(jnp.int32, (1, 128), 1) < 64

    def natural(parts):
        tiles = [[parts[4 + x_][:, q * 128:(q + 1) * 128] for q in (0, 1)] for x_ in range(4)]
        result = list(parts[:4])
        for y_ in range(4):
            for p in (0, 1):
                a, b = tiles[2 * p][y_ // 2], tiles[2 * p + 1][y_ // 2]
                if y_ % 2 == 0:
                    result.append(jnp.where(low, a, pltpu.roll(b, 64, 1)))
                else:
                    result.append(jnp.where(low, pltpu.roll(a, 64, 1), b))
        return jnp.concatenate(result, axis=1)

    def normed(base, arrived, gain, s, target):
        step_rows = 32

        def step(i, _):
            rows = pl.ds(pl.multiple_of(s * SEQ + i * step_rows, step_rows), step_rows)
            v = SCALE * base[0, rows, :].astype(F32) + arrived(rows)
            center = v - jnp.mean(v, axis=-1, keepdims=True)
            spread = jnp.mean(center * center, axis=-1, keepdims=True)
            target[0, rows, :] = (center * lax.rsqrt(spread + EPS) * gain[...]).astype(BF16)
            return 0

        lax.fori_loop(0, SEQ // step_rows, step, 0)

    def expand(g, s=None):
        rows = pl.ds(0, TOK) if s is None else seq(s)

        def step(j, _):
            cols = pl.ds(pl.multiple_of(j * 512, 512), 512)
            raised = jnp.maximum(jnp.dot(f[g, rows, :], wu[:, :, :, cols].reshape(D, 512), preferred_element_type=F32), 0.0)
            hid[g, rows, cols] = (raised * raised).astype(BF16)
            return 0

        lax.fori_loop(0, HID // 512, step, 0)

    barrier = pltpu.get_barrier_semaphore()
    for other in (x_plus, x_minus, y_plus, y_minus, above, below, sibling):
        pl.semaphore_signal(barrier, inc=1, device_id=other, device_id_type=MESH)
    own_tokens = pltpu.make_async_copy(tok, x.at[0], sx_own)
    for which in range(6):
        load(which).start()
    own_tokens.start()
    for t in range(3):
        cast(t)
    pl.semaphore_wait(barrier, 7)

    start_z(MIXER)
    g0_own(MIXER)
    tok_z(0).start()
    tok_sibling().start()
    start_z(UP)
    tok_z(1).start()
    tok_z(2).start()
    start_z(DOWN)
    g0_other(MIXER)
    g1(MIXER)
    g3(MIXER, 0)
    relay_tokens(0)
    g2(MIXER)
    for color in (0, 1):
        mix_swap(0, color).start()
    g3(MIXER, 1)
    relay_tokens(1)
    g3(MIXER, 2)
    relay_tokens(2)
    g3(MIXER, 3)
    for k in (1, 2):
        for color in (0, 1):
            mix_swap(k, color).start()
    g0_own(UP)
    g0_other(UP)
    for s in range(NSEQ):
        tok_relay(s).wait_recv()
    tok_sibling().wait_recv()
    own_tokens.wait()
    g4(MIXER)
    for color in (0, 1):
        mix_swap(3, color).start()
    project(3)
    mixed_copy(1).start()
    g1(UP)
    g3(UP, 0)
    project(2)
    mixed_copy(0).start()
    g2(UP)
    g3(UP, 1)
    project(1)
    g3(UP, 2)
    g3(UP, 3)
    g0_own(DOWN)
    g0_other(DOWN)
    project(0)
    for k in range(4):
        for color in (0, 1):
            mix_swap(k, color).wait_recv()
    mixed_copy(1).wait_recv()
    mixed_copy(0).wait_recv()
    for j in range(NCOL):
        mix_sums(j)
    for j in range(NCOL):
        part_copy(0, 0, j, j).wait_recv()

    def mixing(rows):
        return jnp.concatenate([acc[j, rows, :] + d_recv[0, j, rows, :].astype(F32) for j in range(NCOL)], axis=1)

    for s in range(NSEQ):
        normed(x, mixing, gain1, s, f)
        first_copy(1, s).start()
        first_copy(0, s).start()
    g4(UP)
    g1(DOWN)
    g3(DOWN, 0)
    expand(0)
    g2(DOWN)
    for s in range(NSEQ):
        first_copy(0, s).wait_recv()
    expand(1)
    g3(DOWN, 1)
    all_sent(d_send.at[0], sd_send.at[0, 0])
    for s in range(NSEQ):
        first_copy(1, s).wait_recv()
        first_copy(2, s).start()
        expand(2, s)
        if s == 0:
            g3(DOWN, 2)
        if s == 1:
            g3(DOWN, 3)
        first_copy(2, s).wait_recv()
        expand(3, s)
    pieces = [(k, color) for k in range(4) for color in (0, 1)]
    for n, (k, color) in enumerate(pieces):
        if n == 6:
            ffn_sums(0, 0, 0)
            ffn_sums(0, 0, 1)
            g4(DOWN)
        ffn_sums(2, k, color)
        if n in (0, 6):
            continue
        ffn_send(*pieces[n - 1])
        if n == 5:
            ffn_send(*pieces[5])
    ffn_send(*pieces[7])
    for k in (1, 2, 3):
        for color in (0, 1):
            ffn_sums(0, k, color)
    for k, color in pieces:
        part_copy(1, 0, k * 2 + color, color * 4 + chunk(color, k)).wait_recv()
        sum_copy(k, color).wait_recv()

    def lowered(rows):
        return natural([
            acc[j, rows, :] + d_recv[0, j, rows, :].astype(F32) + z_recv[j, rows, :].astype(F32) for j in range(NCOL)
        ])

    results = []
    for s in range(NSEQ):
        normed(f, lowered, gain2, s, x)
        results.append(pltpu.make_async_copy(x.at[0, seq(s)], out.at[seq(s)], s_out.at[s]))
        results[-1].start()

    for t in range(3):
        all_sent(weights[t].at[pl.ds(0, 7)], sw_send.at[t, 0])
        all_sent(weights[t].at[0, pl.ds(0, 2)], sw_send.at[t, 1])
        zcopy(t, 0, own_row, above).wait_send()
        zcopy(t, 1, own_row, below).wait_send()
    for kind in range(3):
        all_sent(x.at[0], sx_send.at[kind])
        all_sent(f.at[0], sf_send.at[kind])
    for k in range(4):
        for color in (0, 1):
            mix_swap(k, color).wait_send()
    for i in (0, 1):
        mixed_copy(i).wait_send()
        all_sent(d_send.at[i], sd_send.at[1, i])
    all_sent(z_send, sr_send)
    for result in results:
        result.wait()


def local(tokens, outer_weight, inner_weight, value_weight, conv_taps, mix_out, norm_first, up_weight, down_weight, norm_second):
    hbm = pl.BlockSpec(memory_space=pl.ANY)
    vmem = pl.BlockSpec(memory_space=pltpu.VMEM)
    dma = pltpu.SemaphoreType.DMA
    return pl.pallas_call(
        kernel,
        name="mixer_ffn",
        out_shape=jax.ShapeDtypeStruct((TOK, D), BF16),
        in_specs=[hbm] * 7 + [vmem] * 3,
        out_specs=hbm,
        scratch_shapes=[pltpu.VMEM((8, 4, ROWS, w), BF16) for w in WIDTHS]
        + [pltpu.VMEM((8, 4, ROWS, CH), BF16)]
        + [pltpu.VMEM((ROWS, w), BF16) for w in WIDTHS]
        + [
            pltpu.VMEM((4, ROWS, 2 * CH), F32),
            pltpu.VMEM((ROWS, 2 * HID), F32),
            pltpu.VMEM((ROWS, 2 * HID), F32),
            pltpu.VMEM((4, TOK, D), BF16),
            pltpu.VMEM((4, TOK, D), BF16),
            pltpu.VMEM((4, TOK, CH), BF16),
            pltpu.VMEM((2, TOK, CH), BF16),
            pltpu.VMEM((4, TOK, HID), BF16),
            pltpu.VMEM((TOK, 768), F32),
            pltpu.VMEM((2, NCOL, TOK, COLS), BF16),
            pltpu.VMEM((2, NCOL, TOK, COLS), BF16),
            pltpu.VMEM((NCOL, TOK, COLS), BF16),
            pltpu.VMEM((NCOL, TOK, COLS), BF16),
            pltpu.VMEM((NCOL, TOK, COLS), F32),
            pltpu.VMEM((2, 2, TOK, COLS), F32),
            dma((6,)),
            dma((3, 2)),
            dma((3, 2, 20)),
            dma((3, 2)),
            dma((3, 2)),
            dma,
            dma((3,)),
            dma((7,)),
            dma((3,)),
            dma((3, 3)),
            dma((4, 2)),
            dma((4, 2)),
            dma((2,)),
            dma((2,)),
            dma((2, 2)),
            dma((2, 2, 8)),
            dma,
            dma((8,)),
            dma((3,)),
        ],
        compiler_params=pltpu.CompilerParams(
            collective_id=0, has_side_effects=True, vmem_limit_bytes=62 * 1024 * 1024
        ),
    )(
        tokens, outer_weight, inner_weight, value_weight, mix_out.T, up_weight, down_weight.T,
        conv_taps, norm_first.reshape(1, D), norm_second.reshape(1, D),
    )


def solution(mesh):
    finer = Mesh(
        mesh.devices.reshape(mesh.shape["rep"], 2, 4, 4, mesh.shape["tp"]),
        ("rep", "fs_0", "fs_1", "fs_2", "tp"),
    )
    placed = (
        P(REP_FS_TP, None),
        P(FS, "tp"),
        P(FS, "tp"),
        P(FS, "tp"),
        P(None, "tp"),
        P("tp", FS),
        P(),
        P(FS, "tp"),
        P("tp", FS),
        P(),
    )
    return jax.shard_map(
        local, mesh=finer, in_specs=placed, out_specs=P(REP_FS_TP, None), check_vma=False
    )
```

```python
import jax
import jax.numpy as jnp
from jax import lax
from jax.experimental import pallas as pl
from jax.experimental.pallas import tpu as pltpu
from jax.sharding import Mesh
from jax.sharding import PartitionSpec as P

SEQ = 128
FS = ("fs_0", "fs_1", "fs_2")
REP_FS_TP = ("rep", "fs_0", "fs_1", "fs_2", "tp")
MESH = pl.DeviceIdType.MESH
SCALE = 2.0**0.25
EPS = 1e-05
F32 = jnp.float32
BF16 = jnp.bfloat16

D = 2048
ROWS = 64
TOK = 384
CH = 384
HID = 1024
NSEQ = TOK // SEQ
WIDTHS = (4 * CH, HID, HID)
MIXER, UP, DOWN = range(3)
COLS = 256
NCOL = D // COLS


def kernel(
    tok, wo_in, wi_in, wv_in, wm_in, wu_in, wd_in, taps, gain1, gain2, out,
    wp, wu, wd, wm2, gp, gu, gd,
    own, x, f, mixed, mixed2, hid, pd, d_send, d_recv, z_send, z_recv, acc, held,
    s_in, sw_send, sw_recv, sz_send, sz_recv, sx_own, sx_send, sx_recv, sf_send, sf_recv,
    sq_send, sq_recv, sm_send, sm_recv, sd_send, sd_recv, sr_send, sr_recv, s_out,
):
    rep, zl = lax.axis_index("rep"), lax.axis_index("fs_0")
    my_y, my_x, core = lax.axis_index("fs_1"), lax.axis_index("fs_2"), lax.axis_index("tp")
    z = rep * 2 + zl

    def device(z_, y_, x_, c_):
        return (z_ // 2, z_ % 2, y_, x_, c_)

    z_plus, z_minus = (z + 1) % 4, (z + 3) % 4
    above, below = device(z_plus, my_y, my_x, core), device(z_minus, my_y, my_x, core)
    sibling = device(z, my_y, my_x, 1 - core)
    z_to = (z + 3 + 2 * core) % 4
    z_from = (z + 1 + 2 * core) % 4
    helper, helped = device(z_to, my_y, my_x, core), device(z_from, my_y, my_x, core)
    x_plus, x_minus = device(z, my_y, (my_x + 1) % 4, core), device(z, my_y, (my_x + 3) % 4, core)
    y_plus, y_minus = device(z, (my_y + 1) % 4, my_x, core), device(z, (my_y + 3) % 4, my_x, core)

    def remote(src, dst, send_sem, recv_sem, target):
        return pltpu.make_async_remote_copy(
            src_ref=src, dst_ref=dst, send_sem=send_sem, recv_sem=recv_sem, device_id=target, device_id_type=MESH
        )

    weights = (wp, wu, wd)
    given = (gp, gu, gd)
    own_row = (zl * 4 + my_y, my_x)
    other_row = ((1 - zl) * 4 + my_y, my_x)

    def stage(which, width):
        return pd.at[pl.ds(pl.multiple_of(which * ROWS, ROWS), ROWS), pl.ds(0, width)]

    def load(which):
        if which < 4:
            source = (wo_in, wi_in, wv_in, wm_in)[which]
        else:
            source = (wu_in, wd_in)[which // 2 - 2].at[:, pl.ds(which % 2 * HID, HID)]
        return pltpu.make_async_copy(source, stage(which, 2 * CH if which < 4 else HID), s_in.at[which])

    def cast(t):
        keep, give = weights[t].at[own_row[0], own_row[1]], given[t]
        if t == MIXER:
            for which in range(4):
                load(which).wait()
            pieces = [(i, c0, at + i * width, width) for width, c0, at in ((256, 0, 0), (128, 256, 768)) for i in range(3)]
            for i, c0, at, width in pieces + [(3, 0, 3 * CH, CH)]:
                kept = pl.ds(pl.multiple_of(zl * CH + c0, 128), width)
                passed = pl.ds(pl.multiple_of((1 - zl) * CH + c0, 128), width)
                keep[:, at:at + width] = pd[i * ROWS:(i + 1) * ROWS, kept].astype(BF16)
                give[:, at:at + width] = pd[i * ROWS:(i + 1) * ROWS, passed].astype(BF16)
        else:
            first = 2 + 2 * t
            load(first).wait()
            load(first + 1).wait()
            keep[...] = stage(first + zl, HID)[...].astype(BF16)
            give[...] = stage(first + 1 - zl, HID)[...].astype(BF16)

    SHIFT = (0, 3, 1, 2)
    HALF = ROWS // 2
    mine, theirs = zl, 1 - zl

    def block(color, k1, k2):
        y_ = (my_y + SHIFT[k1] * color + SHIFT[k2] * (1 - color)) % 4
        x_ = (my_x + SHIFT[k1] * (1 - color) + SHIFT[k2] * color) % 4
        return (color * 4 + y_, x_)

    def ring(color, leg, step):
        along_y = color if leg == 1 else 1 - color
        return device(z, (my_y + step * along_y) % 4, (my_x + step * (1 - along_y)) % 4, core)

    def wcopy(t, color, slot, row, start, rows, target):
        part = weights[t].at[row[0], row[1], pl.ds(start, rows)]
        return remote(part, part, sw_send.at[t, int(slot == 0)], sw_recv.at[t, color, slot], target)

    def arrive(t, color, slot, row, start, rows):
        wcopy(t, color, slot, row, start, rows, x_plus).wait_recv()

    def first_leg(t, color):
        row = block(color, 0, 0)
        wcopy(t, color, 0, row, 0, ROWS, ring(color, 1, 1)).start()
        wcopy(t, color, 1, row, 0, ROWS, ring(color, 1, 3)).start()

    def second_leg(t, color, k):
        row = block(color, k, 0)
        wcopy(t, color, 4 + 4 * k, row, 0, ROWS, ring(color, 2, 1)).start()
        wcopy(t, color, 5 + 4 * k, row, 0, ROWS, ring(color, 2, 3)).start()

    def zcopy(t, half, row, target):
        return remote(
            given[t].at[pl.ds(half * HALF, HALF)], weights[t].at[row[0], row[1], pl.ds(half * HALF, HALF)],
            sz_send.at[t, half], sz_recv.at[t, half], target,
        )

    def start_z(t):
        zcopy(t, 0, own_row, above).start()
        zcopy(t, 1, own_row, below).start()

    def z_arrived(t):
        zcopy(t, 0, other_row, above).wait_recv()
        zcopy(t, 1, other_row, below).wait_recv()

    def g1(t, color):
        row = block(color, 1, 0)
        arrive(t, color, 0, row, 0, ROWS)
        wcopy(t, color, 2, row, 0, HALF, ring(color, 1, 1)).start()
        row = block(color, 2, 0)
        arrive(t, color, 1, row, 0, ROWS)
        wcopy(t, color, 3, row, HALF, HALF, ring(color, 1, 3)).start()

    def g2(t, color):
        row = block(color, 3, 0)
        arrive(t, color, 2, row, 0, HALF)
        arrive(t, color, 3, row, HALF, HALF)

    def g3(t, color, k):
        row = block(color, k, 1)
        arrive(t, color, 4 + 4 * k, row, 0, ROWS)
        wcopy(t, color, 6 + 4 * k, row, 0, HALF, ring(color, 2, 1)).start()
        row = block(color, k, 2)
        arrive(t, color, 5 + 4 * k, row, 0, ROWS)
        wcopy(t, color, 7 + 4 * k, row, HALF, HALF, ring(color, 2, 3)).start()

    def g4(t):
        for k in range(4):
            for color in (mine, theirs):
                row = block(color, k, 3)
                arrive(t, color, 6 + 4 * k, row, 0, HALF)
                arrive(t, color, 7 + 4 * k, row, HALF, HALF)

    def chunk(color, k):
        return ((my_y, my_x)[color] + SHIFT[k]) % 4

    def chunk_rows(ref, color, at):
        return ref.at[at] if color == 0 else ref.at[pl.ds(4, 4), at]

    def mix_swap(k, color):
        source = chunk_rows(wp, color, chunk(color, k)).at[:, :, pl.ds(3 * CH, CH)]
        return remote(
            source, chunk_rows(wm2, color, chunk(color, k)), sq_send.at[k, color], sq_recv.at[k, color], (above, below)[color]
        )

    def seq(s):
        return pl.ds(s * SEQ, SEQ)

    def tok_z(s):
        return remote(x.at[0, :, seq(s)], x.at[2, :, seq(s)], sx_send.at[0], sx_recv.at[1 + s], helper)

    def tok_sibling():
        return remote(x.at[0], x.at[1], sx_send.at[1], sx_recv.at[0], sibling)

    def tok_relay(s):
        return remote(x.at[2, :, seq(s)], x.at[3, :, seq(s)], sx_send.at[2], sx_recv.at[4 + s], sibling)

    def first_copy(kind, s):
        source, target, to = ((0, 1, sibling), (0, 2, helper), (2, 3, sibling))[kind]
        return remote(f.at[source, seq(s)], f.at[target, seq(s)], sf_send.at[kind], sf_recv.at[kind, s], to)

    def mixed_copy(i):
        return remote(mixed.at[2 + i], mixed2.at[i], sm_send.at[i], sm_recv.at[i], (helped, helper)[i])

    def mix_copy(s):
        rows = (0, slice(None), seq(s))
        return remote(d_send.at[rows], d_recv.at[rows], sd_send.at[0, 0], sd_recv.at[0, 0, s], sibling)

    def piece(k, color, s):
        j = color * 4 + chunk(color, k)
        return j, pl.ds(0, TOK) if s is None else seq(s), (k * 2 + color) * NSEQ + (s or 0)

    def part_copy(slot, k, color, s=None):
        j, rows, at = piece(k, color, s)
        return remote(d_send.at[slot, j, rows], d_recv.at[slot, j, rows], sd_send.at[1, slot], sd_recv.at[1, slot, at], sibling)

    def sum_copy(k, color, s=None):
        j, rows, at = piece(k, color, s)
        return remote(z_send.at[j, rows], z_recv.at[j, rows], sr_send, sr_recv.at[at], helped)

    def relay_tokens(s):
        tok_z(s).wait_recv()
        tok_relay(s).start()

    def all_sent(ref, sem):
        remote(ref, ref, sem, sw_recv.at[0, 0, 0], x_plus).wait_send()

    row_id = lax.broadcasted_iota(jnp.int32, (SEQ, 1), 0)

    low = lax.broadcasted_iota(jnp.int32, (1, 128), 1) < 64

    def spread_tokens():
        for j in range(4):
            x[0, j] = own[:, j * COLS:(j + 1) * COLS]
        for x_ in range(4):
            for q in (0, 1):
                a, b = (
                    own[:, pl.ds(1024 + y_ * COLS + (x_ // 2) * 128, 128)].astype(F32) for y_ in (2 * q, 2 * q + 1)
                )
                if x_ % 2 == 0:
                    joined = jnp.where(low, a, pltpu.roll(b, 64, 1))
                else:
                    joined = jnp.where(low, pltpu.roll(a, 64, 1), b)
                x[0, 4 + x_, :, q * 128:(q + 1) * 128] = joined.astype(BF16)

    def project(p, k):
        rows = pl.ds(p * 2 * TOK, 2 * TOK)
        j0, j1 = chunk(0, k), chunk(1, k)
        for a, b in ((0, 768), (768, 1152)):
            total = jnp.dot(
                x[2 * p:2 * p + 2, j0].reshape(2 * TOK, COLS), wp[j0, :, :, a:b].reshape(COLS, b - a),
                preferred_element_type=F32,
            ) + jnp.dot(
                x[2 * p:2 * p + 2, 4 + j1].reshape(2 * TOK, COLS), wp[4:8, j1, :, a:b].reshape(COLS, b - a),
                preferred_element_type=F32,
            )
            if k == 0:
                pd[rows, a:b] = total
            else:
                pd[rows, a:b] += total

    def convolve(g):
        for ch, c0, at in ((256, 0, 0), (128, 256, 768)):
            tap = [taps[k:k + 1, pl.ds(pl.multiple_of(zl * CH + c0, 128), ch)] for k in range(3)]
            for s in range(NSEQ):
                rows = pl.ds(g * TOK + s * SEQ, SEQ)
                product = pd[rows, pl.ds(at + ch, ch)] * pd[rows, pl.ds(at + 2 * ch, ch)]
                before = jnp.where(row_id > 0, pltpu.roll(product, 1, 0), 0.0)
                after = jnp.where(row_id < SEQ - 1, pltpu.roll(product, SEQ - 1, 0), 0.0)
                conv = tap[0] * before + tap[1] * product + tap[2] * after
                mixed[g, seq(s), c0:c0 + ch] = (pd[rows, pl.ds(at, ch)] * conv).astype(BF16)

    def dot_t(rows, w):
        return lax.dot_general(
            rows, w.reshape(COLS, w.shape[-1]), (((1,), (1,)), ((), ())), preferred_element_type=F32
        )

    def mix_sums(s):
        rows = seq(s)
        left, right = mixed[0:2, rows, :].reshape(2 * SEQ, CH), mixed2[0:2, rows, :].reshape(2 * SEQ, CH)
        for j in range(NCOL):
            total = dot_t(left, wp[j, :, :, 3 * CH:4 * CH]) + dot_t(right, wm2[j])
            acc[j, rows, :] = total[:SEQ]
            d_send[0, j, rows, :] = total[SEQ:].astype(BF16)
        mix_copy(s).start()

    def ffn_sums(p, k, s=None):
        rows = pl.ds(0, TOK) if s is None else seq(s)
        half = TOK if s is None else SEQ
        for color in (0, 1):
            j = color * 4 + chunk(color, k)
            w = wd[j] if color == 0 else wd[4:8, j - 4]
            total = dot_t(hid[2 * p:2 * p + 2, rows, :].reshape(2 * half, HID), w)
            d_send[p, j, rows, :] = total[half:].astype(BF16)
            if p == 0:
                acc[j, rows, :] = total[:half]
            else:
                held[k % 2, color, rows, :] = total[:half]
        for color in (0, 1):
            part_copy(p, k, color, s).start()

    def ffn_send(k, s=None):
        for color in (0, 1):
            if k < 3:
                part_copy(1, k, color, s).wait_recv()
        for color in (0, 1):
            j, rows, _ = piece(k, color, s)
            z_send[j, rows, :] = (held[k % 2, color, rows, :] + d_recv[1, j, rows, :].astype(F32)).astype(BF16)
        for color in (0, 1):
            sum_copy(k, color, s).start()

    def natural(parts):
        tiles = [[parts[4 + x_][:, q * 128:(q + 1) * 128] for q in (0, 1)] for x_ in range(4)]
        result = list(parts[:4])
        for y_ in range(4):
            for p in (0, 1):
                a, b = tiles[2 * p][y_ // 2], tiles[2 * p + 1][y_ // 2]
                if y_ % 2 == 0:
                    result.append(jnp.where(low, a, pltpu.roll(b, 64, 1)))
                else:
                    result.append(jnp.where(low, pltpu.roll(a, 64, 1), b))
        return jnp.concatenate(result, axis=1)

    def normed(base, arrived, gain, s, target):
        step_rows = 32

        def step(i, _):
            rows = pl.ds(pl.multiple_of(s * SEQ + i * step_rows, step_rows), step_rows)
            v = SCALE * base[rows, :].astype(F32) + arrived(rows)
            center = v - jnp.mean(v, axis=-1, keepdims=True)
            spread = jnp.mean(center * center, axis=-1, keepdims=True)
            target[rows, :] = (center * lax.rsqrt(spread + EPS) * gain[...]).astype(BF16)
            return 0

        lax.fori_loop(0, SEQ // step_rows, step, 0)

    def expand(g, s=None):
        rows = pl.ds(0, TOK) if s is None else seq(s)

        def step(j, _):
            cols = pl.ds(pl.multiple_of(j * 512, 512), 512)
            raised = jnp.maximum(jnp.dot(f[g, rows, :], wu[:, :, :, cols].reshape(D, 512), preferred_element_type=F32), 0.0)
            hid[g, rows, cols] = (raised * raised).astype(BF16)
            return 0

        lax.fori_loop(0, HID // 512, step, 0)

    barrier = pltpu.get_barrier_semaphore()
    for other in (x_plus, x_minus, y_plus, y_minus, above, below, sibling):
        pl.semaphore_signal(barrier, inc=1, device_id=other, device_id_type=MESH)
    own_tokens = pltpu.make_async_copy(tok, own, sx_own)
    for which in range(4):
        load(which).start()
    own_tokens.start()
    for which in range(4, 8):
        load(which).start()
    cast(MIXER)
    own_tokens.wait()
    spread_tokens()
    cast(UP)
    cast(DOWN)
    pl.semaphore_wait(barrier, 7)

    both = (mine, theirs)

    def each(step, t, *rest):
        for color in both:
            step(t, color, *rest)

    start_z(MIXER)
    first_leg(MIXER, mine)
    second_leg(MIXER, mine, 0)
    tok_z(0).start()
    tok_sibling().start()
    start_z(UP)
    tok_z(1).start()
    tok_z(2).start()
    start_z(DOWN)
    z_arrived(MIXER)
    first_leg(MIXER, theirs)
    second_leg(MIXER, theirs, 0)
    g1(MIXER, mine)
    second_leg(MIXER, mine, 1)
    relay_tokens(0)
    g1(MIXER, theirs)
    second_leg(MIXER, mine, 2)
    second_leg(MIXER, theirs, 1)
    second_leg(MIXER, theirs, 2)
    g2(MIXER, mine)
    second_leg(MIXER, mine, 3)
    g2(MIXER, theirs)
    second_leg(MIXER, theirs, 3)
    for color in (0, 1):
        mix_swap(0, color).start()
    each(g3, MIXER, 0)
    relay_tokens(1)
    tok_sibling().wait_recv()
    project(0, 0)
    each(g3, MIXER, 1)
    relay_tokens(2)
    each(g3, MIXER, 2)
    for s in range(NSEQ):
        tok_relay(s).wait_recv()
    project(1, 0)
    each(g3, MIXER, 3)
    z_arrived(UP)
    each(first_leg, UP)
    each(second_leg, UP, 0)
    for k in (1, 2):
        for color in (0, 1):
            mix_swap(k, color).start()
    project(1, 1)
    project(1, 2)
    g4(MIXER)
    for color in (0, 1):
        mix_swap(3, color).start()
    project(1, 3)
    convolve(3)
    mixed_copy(1).start()
    convolve(2)
    mixed_copy(0).start()
    each(g1, UP)
    each(second_leg, UP, 1)
    z_arrived(DOWN)
    each(first_leg, DOWN)
    each(second_leg, UP, 2)
    project(0, 1)
    each(g3, UP, 0)
    project(0, 2)
    each(g2, UP)
    each(second_leg, UP, 3)
    project(0, 3)
    convolve(1)
    convolve(0)
    each(g1, DOWN)
    each(g3, UP, 1)
    for k in range(4):
        for color in (0, 1):
            mix_swap(k, color).wait_recv()
    mixed_copy(1).wait_recv()
    mixed_copy(0).wait_recv()

    def mixing(rows):
        return jnp.concatenate([acc[j, rows, :] + d_recv[0, j, rows, :].astype(F32) for j in range(NCOL)], axis=1)

    def make_first(s):
        mix_copy(s).wait_recv()
        normed(own, mixing, gain1, s, f.at[0])
        first_copy(1, s).start()
        first_copy(0, s).start()

    mix_sums(0)
    each(g3, UP, 2)
    mix_sums(1)
    make_first(0)
    mix_sums(2)
    each(g3, UP, 3)
    for k in (0, 1, 2):
        each(second_leg, DOWN, k)
    make_first(1)
    make_first(2)
    each(g2, DOWN)
    each(second_leg, DOWN, 3)
    g4(UP)
    expand(0)
    each(g3, DOWN, 0)
    for s in range(NSEQ):
        first_copy(0, s).wait_recv()
    expand(1)
    all_sent(d_send.at[0], sd_send.at[0, 0])
    for s in range(NSEQ):
        first_copy(1, s).wait_recv()
        first_copy(2, s).start()
        expand(2, s)
        if s > 0:
            ffn_send(0, s - 1)
        first_copy(2, s).wait_recv()
        expand(3, s)
        ffn_sums(1, 0, s)
        each(g3, DOWN, s + 1)
    ffn_sums(1, 1)
    ffn_send(0, 2)
    ffn_sums(1, 2)
    ffn_send(1)
    ffn_sums(0, 0)
    ffn_send(2)
    g4(DOWN)
    ffn_sums(1, 3)
    ffn_sums(0, 1)
    for color in (0, 1):
        part_copy(1, 3, color).wait_recv()
    for s in range(NSEQ):
        ffn_send(3, s)
    ffn_sums(0, 2)
    ffn_sums(0, 3)
    for k in range(4):
        for color in (0, 1):
            part_copy(0, k, color).wait_recv()
            if k == 0:
                for s in range(NSEQ):
                    sum_copy(k, color, s).wait_recv()
            elif k < 3:
                sum_copy(k, color).wait_recv()

    def lowered(rows):
        return natural([
            acc[j, rows, :] + d_recv[0, j, rows, :].astype(F32) + z_recv[j, rows, :].astype(F32) for j in range(NCOL)
        ])

    results = []
    for s in range(NSEQ):
        for color in (0, 1):
            sum_copy(3, color, s).wait_recv()
        normed(f.at[0], lowered, gain2, s, own)
        results.append(pltpu.make_async_copy(own.at[seq(s)], out.at[seq(s)], s_out.at[s]))
        results[-1].start()

    for t in range(3):
        all_sent(weights[t].at[pl.ds(0, 7)], sw_send.at[t, 0])
        all_sent(weights[t].at[0, pl.ds(0, 2)], sw_send.at[t, 1])
        zcopy(t, 0, own_row, above).wait_send()
        zcopy(t, 1, own_row, below).wait_send()
    for kind in range(3):
        all_sent(x.at[0], sx_send.at[kind])
        all_sent(f.at[0], sf_send.at[kind])
    for k in range(4):
        for color in (0, 1):
            mix_swap(k, color).wait_send()
    for i in (0, 1):
        mixed_copy(i).wait_send()
        all_sent(d_send.at[i], sd_send.at[1, i])
    all_sent(z_send, sr_send)
    for result in results:
        result.wait()


def local(tokens, outer_weight, inner_weight, value_weight, conv_taps, mix_out, norm_first, up_weight, down_weight, norm_second):
    hbm = pl.BlockSpec(memory_space=pl.ANY)
    vmem = pl.BlockSpec(memory_space=pltpu.VMEM)
    dma = pltpu.SemaphoreType.DMA
    return pl.pallas_call(
        kernel,
        name="mixer_ffn",
        out_shape=jax.ShapeDtypeStruct((TOK, D), BF16),
        in_specs=[hbm] * 7 + [vmem] * 3,
        out_specs=hbm,
        scratch_shapes=[pltpu.VMEM((8, 4, ROWS, w), BF16) for w in WIDTHS]
        + [pltpu.VMEM((8, 4, ROWS, CH), BF16)]
        + [pltpu.VMEM((ROWS, w), BF16) for w in WIDTHS]
        + [
            pltpu.VMEM((TOK, D), BF16),
            pltpu.VMEM((4, 8, TOK, COLS), BF16),
            pltpu.VMEM((4, TOK, D), BF16),
            pltpu.VMEM((4, TOK, CH), BF16),
            pltpu.VMEM((2, TOK, CH), BF16),
            pltpu.VMEM((4, TOK, HID), BF16),
            pltpu.VMEM((4 * TOK, 3 * CH), F32),
            pltpu.VMEM((2, NCOL, TOK, COLS), BF16),
            pltpu.VMEM((2, NCOL, TOK, COLS), BF16),
            pltpu.VMEM((NCOL, TOK, COLS), BF16),
            pltpu.VMEM((NCOL, TOK, COLS), BF16),
            pltpu.VMEM((NCOL, TOK, COLS), F32),
            pltpu.VMEM((2, 2, TOK, COLS), F32),
            dma((8,)),
            dma((3, 2)),
            dma((3, 2, 20)),
            dma((3, 2)),
            dma((3, 2)),
            dma,
            dma((3,)),
            dma((7,)),
            dma((3,)),
            dma((3, 3)),
            dma((4, 2)),
            dma((4, 2)),
            dma((2,)),
            dma((2,)),
            dma((2, 2)),
            dma((2, 2, 24)),
            dma,
            dma((24,)),
            dma((3,)),
        ],
        compiler_params=pltpu.CompilerParams(
            collective_id=0, has_side_effects=True, vmem_limit_bytes=67_043_328
        ),
    )(
        tokens, outer_weight, inner_weight, value_weight, mix_out.T, up_weight, down_weight.T,
        conv_taps, norm_first.reshape(1, D), norm_second.reshape(1, D),
    )


def solution(mesh):
    finer = Mesh(
        mesh.devices.reshape(mesh.shape["rep"], 2, 4, 4, mesh.shape["tp"]),
        ("rep", "fs_0", "fs_1", "fs_2", "tp"),
    )
    placed = (
        P(REP_FS_TP, None),
        P(FS, "tp"),
        P(FS, "tp"),
        P(FS, "tp"),
        P(None, "tp"),
        P("tp", FS),
        P(),
        P(FS, "tp"),
        P("tp", FS),
        P(),
    )
    return jax.shard_map(
        local, mesh=finer, in_specs=placed, out_specs=P(REP_FS_TP, None), check_vma=False
    )
```

```python
import jax
import jax.numpy as jnp
from jax import lax
from jax.experimental import pallas as pl
from jax.experimental.pallas import tpu as pltpu
from jax.sharding import Mesh
from jax.sharding import PartitionSpec as P

SEQ = 128
FS = ("fs_0", "fs_1", "fs_2")
REP_FS_TP = ("rep", "fs_0", "fs_1", "fs_2", "tp")
MESH = pl.DeviceIdType.MESH
SCALE = 2.0**0.25
EPS = 1e-05
F32 = jnp.float32
BF16 = jnp.bfloat16

D = 2048
ROWS = 64
TOK = 384
CH = 384
HID = 1024
NSEQ = TOK // SEQ
WIDTHS = (4 * CH, HID, HID)
MIXER, UP, DOWN = range(3)
COLS = 256
NCOL = D // COLS


def kernel(
    tok, wo_in, wi_in, wv_in, wm_in, wu_in, wd_in, taps, gain1, gain2, out,
    wp, wu, wd, wm2, gp, gu, gd,
    own, x, f, mixed, mixed2, hid, pd, d_send, d_recv, z_send, z_recv, acc, held,
    s_in, sw_send, sw_recv, sz_send, sz_recv, sx_own, sx_send, sx_recv, sf_send, sf_recv,
    sq_send, sq_recv, sm_send, sm_recv, sd_send, sd_recv, sr_send, sr_recv, s_out,
):
    rep, zl = lax.axis_index("rep"), lax.axis_index("fs_0")
    my_y, my_x, core = lax.axis_index("fs_1"), lax.axis_index("fs_2"), lax.axis_index("tp")
    z = rep * 2 + zl

    def device(z_, y_, x_, c_):
        return (z_ // 2, z_ % 2, y_, x_, c_)

    z_plus, z_minus = (z + 1) % 4, (z + 3) % 4
    above, below = device(z_plus, my_y, my_x, core), device(z_minus, my_y, my_x, core)
    sibling = device(z, my_y, my_x, 1 - core)
    z_to = (z + 3 + 2 * core) % 4
    z_from = (z + 1 + 2 * core) % 4
    helper, helped = device(z_to, my_y, my_x, core), device(z_from, my_y, my_x, core)
    x_plus, x_minus = device(z, my_y, (my_x + 1) % 4, core), device(z, my_y, (my_x + 3) % 4, core)
    y_plus, y_minus = device(z, (my_y + 1) % 4, my_x, core), device(z, (my_y + 3) % 4, my_x, core)

    def remote(src, dst, send_sem, recv_sem, target):
        return pltpu.make_async_remote_copy(
            src_ref=src, dst_ref=dst, send_sem=send_sem, recv_sem=recv_sem, device_id=target, device_id_type=MESH
        )

    weights = (wp, wu, wd)
    given = (gp, gu, gd)
    own_row = (zl * 4 + my_y, my_x)
    other_row = ((1 - zl) * 4 + my_y, my_x)

    def stage(which, width):
        return pd.at[pl.ds(pl.multiple_of(which * ROWS, ROWS), ROWS), pl.ds(0, width)]

    def load(which):
        if which < 4:
            source = (wo_in, wi_in, wv_in, wm_in)[which]
        else:
            source = (wu_in, wd_in)[which // 2 - 2].at[:, pl.ds(which % 2 * HID, HID)]
        return pltpu.make_async_copy(source, stage(which, 2 * CH if which < 4 else HID), s_in.at[max(which // 2 - 1, 0)])

    def loaded(t):
        part = pd.at[(pl.ds(0, 4 * ROWS), pl.ds(0, 2 * CH))] if t == MIXER else pd.at[pl.ds(2 * ROWS, 2 * ROWS), pl.ds(0, HID)]
        pltpu.make_async_copy(part, part, s_in.at[t]).wait()

    def cast(t):
        keep, give = weights[t].at[own_row[0], own_row[1]], given[t]
        if t == MIXER:
            loaded(t)
            pieces = [(i, c0, at + i * width, width) for width, c0, at in ((256, 0, 0), (128, 256, 768)) for i in range(3)]
            for i, c0, at, width in pieces + [(3, 0, 3 * CH, CH)]:
                kept = pl.ds(pl.multiple_of(zl * CH + c0, 128), width)
                passed = pl.ds(pl.multiple_of((1 - zl) * CH + c0, 128), width)
                keep[:, at:at + width] = pd[i * ROWS:(i + 1) * ROWS, kept].astype(BF16)
                give[:, at:at + width] = pd[i * ROWS:(i + 1) * ROWS, passed].astype(BF16)
        else:
            first = 2 + 2 * t
            loaded(t)
            keep[...] = stage(first + zl, HID)[...].astype(BF16)
            give[...] = stage(first + 1 - zl, HID)[...].astype(BF16)

    SHIFT = (0, 3, 1, 2)
    HALF = ROWS // 2
    mine, theirs = zl, 1 - zl

    def block(color, k1, k2):
        y_ = (my_y + SHIFT[k1] * color + SHIFT[k2] * (1 - color)) % 4
        x_ = (my_x + SHIFT[k1] * (1 - color) + SHIFT[k2] * color) % 4
        return (color * 4 + y_, x_)

    def ring(color, leg, step):
        along_y = color if leg == 1 else 1 - color
        return device(z, (my_y + step * along_y) % 4, (my_x + step * (1 - along_y)) % 4, core)

    def wcopy(t, color, slot, row, start, rows, target, sent=0):
        part = weights[t].at[row[0], row[1], pl.ds(start, rows)]
        return remote(part, part, sw_send.at[t, sent], sw_recv.at[t, color, slot], target)

    def arrive(t, color, slot, blocks):
        part = weights[t].at[0, pl.ds(0, blocks)]
        remote(part, part, sw_send.at[t, 0], sw_recv.at[t, color, slot], x_plus).wait_recv()

    def first_leg(t, color):
        row = block(color, 0, 0)
        wcopy(t, color, 0, row, 0, ROWS, ring(color, 1, 1), 1).start()
        wcopy(t, color, 0, row, 0, ROWS, ring(color, 1, 3)).start()

    def second_leg(t, color, k):
        row = block(color, k, 0)
        wcopy(t, color, 2 + k, row, 0, ROWS, ring(color, 2, 1)).start()
        wcopy(t, color, 2 + k, row, 0, ROWS, ring(color, 2, 3)).start()

    def zcopy(t, half, row, target):
        return remote(
            given[t].at[pl.ds(half * HALF, HALF)], weights[t].at[row[0], row[1], pl.ds(half * HALF, HALF)],
            sz_send.at[t], sz_recv.at[t], target,
        )

    def start_z(t):
        zcopy(t, 0, own_row, above).start()
        zcopy(t, 1, own_row, below).start()

    def z_arrived(t):
        part = weights[t].at[other_row[0], other_row[1]]
        remote(part, part, sz_send.at[t], sz_recv.at[t], above).wait_recv()

    def g1(t, color):
        arrive(t, color, 0, 2)
        wcopy(t, color, 1, block(color, 1, 0), 0, HALF, ring(color, 1, 1)).start()
        wcopy(t, color, 1, block(color, 2, 0), HALF, HALF, ring(color, 1, 3)).start()

    def g2(t, color):
        arrive(t, color, 1, 1)

    def g3(t, color, k):
        arrive(t, color, 2 + k, 2)
        wcopy(t, color, 6, block(color, k, 1), 0, HALF, ring(color, 2, 1)).start()
        wcopy(t, color, 6, block(color, k, 2), HALF, HALF, ring(color, 2, 3)).start()

    def g4(t):
        for color in (mine, theirs):
            arrive(t, color, 6, 4)

    def chunk(color, k):
        return ((my_y, my_x)[color] + SHIFT[k]) % 4

    def chunk_rows(ref, color, at):
        return ref.at[at] if color == 0 else ref.at[pl.ds(4, 4), at]

    def mix_swap(k, color):
        source = chunk_rows(wp, color, chunk(color, k)).at[:, :, pl.ds(3 * CH, CH)]
        return remote(
            source, chunk_rows(wm2, color, chunk(color, k)), sq_send, sq_recv, (above, below)[color]
        )

    def seq(s):
        return pl.ds(s * SEQ, SEQ)

    def tok_z(s):
        return remote(x.at[0, :, seq(s)], x.at[2, :, seq(s)], sx_send, sx_recv.at[1 + s], helper)

    def tok_sibling():
        return remote(x.at[0], x.at[1], sx_send, sx_recv.at[0], sibling)

    def tok_relay(s):
        return remote(x.at[2, :, seq(s)], x.at[3, :, seq(s)], sx_send, sx_recv.at[4], sibling)

    def first_copy(kind, s):
        source, target, to = ((0, 1, sibling), (0, 2, helper), (2, 3, sibling))[kind]
        return remote(f.at[source, seq(s)], f.at[target, seq(s)], sf_send, sf_recv.at[(0, 1 + s, 4 + s)[kind]], to)

    def mixed_copy(i):
        return remote(mixed.at[2 + i], mixed2.at[i], sm_send, sm_recv, (helped, helper)[i])

    def mix_copy(s):
        rows = (0, slice(None), seq(s))
        return remote(d_send.at[rows], d_recv.at[rows], sd_send.at[0], sd_recv.at[s], sibling)

    def piece(k, color, s):
        return color * 4 + chunk(color, k), pl.ds(0, TOK) if s is None else seq(s)

    def part_copy(slot, k, color, s=None):
        j, rows = piece(k, color, s)
        at = 3 if slot == 0 else 4 + 3 * k + s if k < 2 else 8 + k
        return remote(d_send.at[slot, j, rows], d_recv.at[slot, j, rows], sd_send.at[1], sd_recv.at[at], sibling)

    def sum_copy(k, color, s=None):
        j, rows = piece(k, color, s)
        return remote(z_send.at[j, rows], z_recv.at[j, rows], sr_send, sr_recv.at[0 if k < 3 else 1 + s], helped)

    def came(ref, sem):
        remote(ref, ref, sr_send, sem, x_plus).wait_recv()

    def relay_tokens(s):
        tok_z(s).wait_recv()
        tok_relay(s).start()

    def all_sent(ref, sem):
        remote(ref, ref, sem, sr_recv.at[0], x_plus).wait_send()

    row_id = lax.broadcasted_iota(jnp.int32, (SEQ, 1), 0)

    low = lax.broadcasted_iota(jnp.int32, (1, 128), 1) < 64

    def spread_tokens():
        for j in range(4):
            x[0, j] = own[:, j * COLS:(j + 1) * COLS]
        for x_ in range(4):
            for q in (0, 1):
                a, b = (
                    own[:, pl.ds(1024 + y_ * COLS + (x_ // 2) * 128, 128)].astype(F32) for y_ in (2 * q, 2 * q + 1)
                )
                if x_ % 2 == 0:
                    joined = jnp.where(low, a, pltpu.roll(b, 64, 1))
                else:
                    joined = jnp.where(low, pltpu.roll(a, 64, 1), b)
                x[0, 4 + x_, :, q * 128:(q + 1) * 128] = joined.astype(BF16)

    def project(p, k):
        rows = pl.ds(p * 2 * TOK, 2 * TOK)
        j0, j1 = chunk(0, k), chunk(1, k)
        for a, b in ((0, 768), (768, 1152)):
            total = jnp.dot(
                x[2 * p:2 * p + 2, j0].reshape(2 * TOK, COLS), wp[j0, :, :, a:b].reshape(COLS, b - a),
                preferred_element_type=F32,
            ) + jnp.dot(
                x[2 * p:2 * p + 2, 4 + j1].reshape(2 * TOK, COLS), wp[4:8, j1, :, a:b].reshape(COLS, b - a),
                preferred_element_type=F32,
            )
            if k == 0:
                pd[rows, a:b] = total
            else:
                pd[rows, a:b] += total

    def convolve(g):
        for ch, c0, at in ((256, 0, 0), (128, 256, 768)):
            tap = [taps[k:k + 1, pl.ds(pl.multiple_of(zl * CH + c0, 128), ch)] for k in range(3)]
            for s in range(NSEQ):
                rows = pl.ds(g * TOK + s * SEQ, SEQ)
                product = pd[rows, pl.ds(at + ch, ch)] * pd[rows, pl.ds(at + 2 * ch, ch)]
                before = jnp.where(row_id > 0, pltpu.roll(product, 1, 0), 0.0)
                after = jnp.where(row_id < SEQ - 1, pltpu.roll(product, SEQ - 1, 0), 0.0)
                conv = tap[0] * before + tap[1] * product + tap[2] * after
                mixed[g, seq(s), c0:c0 + ch] = (pd[rows, pl.ds(at, ch)] * conv).astype(BF16)

    def dot_t(rows, w):
        return lax.dot_general(
            rows, w.reshape(COLS, w.shape[-1]), (((1,), (1,)), ((), ())), preferred_element_type=F32
        )

    def mix_sums(s):
        rows = seq(s)
        left, right = mixed[0:2, rows, :].reshape(2 * SEQ, CH), mixed2[0:2, rows, :].reshape(2 * SEQ, CH)
        for j in range(NCOL):
            total = dot_t(left, wp[j, :, :, 3 * CH:4 * CH]) + dot_t(right, wm2[j])
            acc[j, rows, :] = total[:SEQ]
            d_send[0, j, rows, :] = total[SEQ:].astype(BF16)
        mix_copy(s).start()

    def ffn_sums(p, k, s=None):
        rows = pl.ds(0, TOK) if s is None else seq(s)
        half = TOK if s is None else SEQ
        for color in (0, 1):
            j = color * 4 + chunk(color, k)
            w = wd[j] if color == 0 else wd[4:8, j - 4]
            total = dot_t(hid[2 * p:2 * p + 2, rows, :].reshape(2 * half, HID), w)
            d_send[p, j, rows, :] = total[half:].astype(BF16)
            if p == 0:
                acc[j, rows, :] = total[:half]
            else:
                held[k % 2, color, rows, :] = total[:half]
        for color in (0, 1):
            part_copy(p, k, color, s).start()

    def ffn_send(k, s=None):
        if k < 3:
            rows = pl.ds(0, TOK) if s is None else seq(s)
            came(d_recv.at[1, pl.ds(0, 2), rows], sd_recv.at[4 + 3 * k + s if k < 2 else 8 + k])
        for color in (0, 1):
            j, rows = piece(k, color, s)
            z_send[j, rows, :] = (held[k % 2, color, rows, :] + d_recv[1, j, rows, :].astype(F32)).astype(BF16)
        for color in (0, 1):
            sum_copy(k, color, s).start()

    def natural(parts):
        tiles = [[parts[4 + x_][:, q * 128:(q + 1) * 128] for q in (0, 1)] for x_ in range(4)]
        result = list(parts[:4])
        for y_ in range(4):
            for p in (0, 1):
                a, b = tiles[2 * p][y_ // 2], tiles[2 * p + 1][y_ // 2]
                if y_ % 2 == 0:
                    result.append(jnp.where(low, a, pltpu.roll(b, 64, 1)))
                else:
                    result.append(jnp.where(low, pltpu.roll(a, 64, 1), b))
        return jnp.concatenate(result, axis=1)

    def normed(base, arrived, gain, s, target):
        step_rows = 32

        def step(i, _):
            rows = pl.ds(pl.multiple_of(s * SEQ + i * step_rows, step_rows), step_rows)
            v = SCALE * base[rows, :].astype(F32) + arrived(rows)
            center = v - jnp.mean(v, axis=-1, keepdims=True)
            spread = jnp.mean(center * center, axis=-1, keepdims=True)
            target[rows, :] = (center * lax.rsqrt(spread + EPS) * gain[...]).astype(BF16)
            return 0

        lax.fori_loop(0, SEQ // step_rows, step, 0)

    def expand(g, s=None):
        rows = pl.ds(0, TOK) if s is None else seq(s)

        def step(j, _):
            cols = pl.ds(pl.multiple_of(j * 512, 512), 512)
            raised = jnp.maximum(jnp.dot(f[g, rows, :], wu[:, :, :, cols].reshape(D, 512), preferred_element_type=F32), 0.0)
            hid[g, rows, cols] = (raised * raised).astype(BF16)
            return 0

        lax.fori_loop(0, HID // 512, step, 0)

    barrier = pltpu.get_barrier_semaphore()
    for other in (x_plus, x_minus, y_plus, y_minus, above, below, sibling):
        pl.semaphore_signal(barrier, inc=1, device_id=other, device_id_type=MESH)
    own_tokens = pltpu.make_async_copy(tok, own, sx_own)
    for which in range(4):
        load(which).start()
    own_tokens.start()
    for which in range(4, 8):
        load(which).start()
    cast(MIXER)
    own_tokens.wait()
    spread_tokens()
    cast(UP)
    cast(DOWN)
    pl.semaphore_wait(barrier, 7)

    both = (mine, theirs)

    def each(step, t, *rest):
        for color in both:
            step(t, color, *rest)

    start_z(MIXER)
    first_leg(MIXER, mine)
    second_leg(MIXER, mine, 0)
    tok_z(0).start()
    tok_sibling().start()
    start_z(UP)
    tok_z(1).start()
    tok_z(2).start()
    start_z(DOWN)
    z_arrived(MIXER)
    first_leg(MIXER, theirs)
    second_leg(MIXER, theirs, 0)
    g1(MIXER, mine)
    second_leg(MIXER, mine, 1)
    relay_tokens(0)
    g1(MIXER, theirs)
    second_leg(MIXER, mine, 2)
    second_leg(MIXER, theirs, 1)
    second_leg(MIXER, theirs, 2)
    g2(MIXER, mine)
    second_leg(MIXER, mine, 3)
    g2(MIXER, theirs)
    second_leg(MIXER, theirs, 3)
    for color in (0, 1):
        mix_swap(0, color).start()
    each(g3, MIXER, 0)
    relay_tokens(1)
    tok_sibling().wait_recv()
    project(0, 0)
    each(g3, MIXER, 1)
    relay_tokens(2)
    each(g3, MIXER, 2)
    came(x.at[3], sx_recv.at[4])
    project(1, 0)
    each(g3, MIXER, 3)
    z_arrived(UP)
    each(first_leg, UP)
    each(second_leg, UP, 0)
    for k in (1, 2):
        for color in (0, 1):
            mix_swap(k, color).start()
    project(1, 1)
    project(1, 2)
    g4(MIXER)
    for color in (0, 1):
        mix_swap(3, color).start()
    project(1, 3)
    convolve(3)
    mixed_copy(1).start()
    convolve(2)
    mixed_copy(0).start()
    each(g1, UP)
    each(second_leg, UP, 1)
    z_arrived(DOWN)
    each(first_leg, DOWN)
    each(second_leg, UP, 2)
    project(0, 1)
    each(g3, UP, 0)
    project(0, 2)
    each(g2, UP)
    each(second_leg, UP, 3)
    project(0, 3)
    convolve(1)
    convolve(0)
    came(wm2, sq_recv)
    came(mixed2, sm_recv)

    def mixing(rows):
        return jnp.concatenate([acc[j, rows, :] + d_recv[0, j, rows, :].astype(F32) for j in range(NCOL)], axis=1)

    def make_first(s):
        mix_copy(s).wait_recv()
        normed(own, mixing, gain1, s, f.at[0])
        first_copy(1, s).start()
        first_copy(0, s).start()

    mix_sums(0)
    each(g3, UP, 1)
    mix_sums(1)
    make_first(0)
    each(g1, DOWN)
    mix_sums(2)
    each(g3, UP, 2)
    make_first(1)
    second_leg(DOWN, mine, 0)
    second_leg(DOWN, theirs, 0)
    make_first(2)
    each(g3, UP, 3)
    for k in (1, 2):
        each(second_leg, DOWN, k)
    each(g2, DOWN)
    each(second_leg, DOWN, 3)
    came(f.at[1], sf_recv.at[0])
    g4(UP)
    expand(0)
    each(g3, DOWN, 0)
    all_sent(d_send.at[0], sd_send.at[0])
    first_copy(1, 0).wait_recv()
    first_copy(2, 0).start()
    expand(2, 0)
    first_copy(2, 0).wait_recv()
    expand(3, 0)
    ffn_sums(1, 0, 0)
    expand(1)
    ffn_send(0, 0)
    each(g3, DOWN, 1)
    first_copy(1, 1).wait_recv()
    first_copy(2, 1).start()
    expand(2, 1)
    each(g3, DOWN, 2)
    first_copy(2, 1).wait_recv()
    expand(3, 1)
    ffn_sums(1, 0, 1)
    each(g3, DOWN, 3)
    ffn_sums(1, 1, 0)
    ffn_send(0, 1)
    ffn_sums(1, 1, 1)
    ffn_send(1, 0)
    first_copy(1, 2).wait_recv()
    first_copy(2, 2).start()
    expand(2, 2)
    ffn_send(1, 1)
    first_copy(2, 2).wait_recv()
    expand(3, 2)
    ffn_sums(1, 0, 2)
    ffn_sums(1, 1, 2)
    ffn_send(0, 2)
    ffn_sums(1, 2)
    ffn_send(1, 2)
    g4(DOWN)
    ffn_sums(1, 3)
    ffn_send(2)
    ffn_sums(0, 0)
    came(d_recv.at[1, pl.ds(0, 2)], sd_recv.at[11])
    for s in range(NSEQ):
        ffn_send(3, s)
    for k in (1, 2, 3):
        ffn_sums(0, k)
    came(d_recv.at[0], sd_recv.at[3])
    came(z_recv.at[pl.ds(0, 6)], sr_recv.at[0])

    def lowered(rows):
        return natural([
            acc[j, rows, :] + d_recv[0, j, rows, :].astype(F32) + z_recv[j, rows, :].astype(F32) for j in range(NCOL)
        ])

    for s in range(NSEQ):
        came(z_recv.at[pl.ds(0, 2), seq(s)], sr_recv.at[1 + s])
        normed(f.at[0], lowered, gain2, s, own)
        pltpu.make_async_copy(own.at[seq(s)], out.at[seq(s)], s_out).start()

    for t in range(3):
        all_sent(weights[t].at[pl.ds(0, 7)], sw_send.at[t, 0])
        all_sent(weights[t].at[0, pl.ds(0, 2)], sw_send.at[t, 1])
        all_sent(given[t], sz_send.at[t])
    all_sent(x.at[pl.ds(0, 3)], sx_send)
    all_sent(f.at[pl.ds(0, 3)], sf_send)
    all_sent(wm2, sq_send)
    all_sent(mixed2, sm_send)
    all_sent(d_send, sd_send.at[1])
    all_sent(z_send, sr_send)
    pltpu.make_async_copy(own, out, s_out).wait()


def local(tokens, outer_weight, inner_weight, value_weight, conv_taps, mix_out, norm_first, up_weight, down_weight, norm_second):
    hbm = pl.BlockSpec(memory_space=pl.ANY)
    vmem = pl.BlockSpec(memory_space=pltpu.VMEM)
    dma = pltpu.SemaphoreType.DMA
    return pl.pallas_call(
        kernel,
        name="mixer_ffn",
        out_shape=jax.ShapeDtypeStruct((TOK, D), BF16),
        in_specs=[hbm] * 7 + [vmem] * 3,
        out_specs=hbm,
        scratch_shapes=[pltpu.VMEM((8, 4, ROWS, w), BF16) for w in WIDTHS]
        + [pltpu.VMEM((8, 4, ROWS, CH), BF16)]
        + [pltpu.VMEM((ROWS, w), BF16) for w in WIDTHS]
        + [
            pltpu.VMEM((TOK, D), BF16),
            pltpu.VMEM((4, 8, TOK, COLS), BF16),
            pltpu.VMEM((4, TOK, D), BF16),
            pltpu.VMEM((4, TOK, CH), BF16),
            pltpu.VMEM((2, TOK, CH), BF16),
            pltpu.VMEM((4, TOK, HID), BF16),
            pltpu.VMEM((4 * TOK, 3 * CH), F32),
            pltpu.VMEM((2, NCOL, TOK, COLS), BF16),
            pltpu.VMEM((2, NCOL, TOK, COLS), BF16),
            pltpu.VMEM((NCOL, TOK, COLS), BF16),
            pltpu.VMEM((NCOL, TOK, COLS), BF16),
            pltpu.VMEM((NCOL, TOK, COLS), F32),
            pltpu.VMEM((2, 2, TOK, COLS), F32),
            dma((3,)),
            dma((3, 2)),
            dma((3, 2, 7)),
            dma((3,)),
            dma((3,)),
            dma,
            dma,
            dma((5,)),
            dma,
            dma((7,)),
            dma,
            dma,
            dma,
            dma,
            dma((2,)),
            dma((12,)),
            dma,
            dma((4,)),
            dma,
        ],
        compiler_params=pltpu.CompilerParams(
            collective_id=0, has_side_effects=True, vmem_limit_bytes=67_043_328
        ),
    )(
        tokens, outer_weight, inner_weight, value_weight, mix_out.T, up_weight, down_weight.T,
        conv_taps, norm_first.reshape(1, D), norm_second.reshape(1, D),
    )


def solution(mesh):
    finer = Mesh(
        mesh.devices.reshape(mesh.shape["rep"], 2, 4, 4, mesh.shape["tp"]),
        ("rep", "fs_0", "fs_1", "fs_2", "tp"),
    )
    placed = (
        P(REP_FS_TP, None),
        P(FS, "tp"),
        P(FS, "tp"),
        P(FS, "tp"),
        P(None, "tp"),
        P("tp", FS),
        P(),
        P(FS, "tp"),
        P("tp", FS),
        P(),
    )
    return jax.shard_map(
        local, mesh=finer, in_specs=placed, out_specs=P(REP_FS_TP, None), check_vma=False
    )
```

```python
import jax
import jax.numpy as jnp
from jax import lax
from jax.experimental import pallas as pl
from jax.experimental.pallas import tpu as pltpu
from jax.sharding import Mesh
from jax.sharding import PartitionSpec as P

SEQ = 128
FS = ("fs_0", "fs_1", "fs_2")
REP_FS_TP = ("rep", "fs_0", "fs_1", "fs_2", "tp")
MESH = pl.DeviceIdType.MESH
SCALE = 2.0**0.25
EPS = 1e-05
F32 = jnp.float32
BF16 = jnp.bfloat16

D = 2048
ROWS = 64
TOK = 384
CH = 384
HID = 1024
NSEQ = TOK // SEQ
WIDTHS = (4 * CH, HID, HID)
MIXER, UP, DOWN = range(3)
COLS = 256
NCOL = D // COLS


def kernel(
    tok, wo_in, wi_in, wv_in, wm_in, wu_in, wd_in, taps_in, gain1_in, gain2_in, own,
    wp, wu, wd, wm2, gp, gu, gd,
    x, f, mixed, mixed2, hid, pd, d_send, d_recv, z_send, z_recv, acc, held, taps, gain1, gain2,
    s_small, s_in, sw_send, sw_recv, sz_send, sz_recv, sx_own, sx_send, sx_recv, sf_send, sf_recv,
    sq_send, sq_recv, sm_send, sm_recv, sd_send, sd_recv, sr_send, sr_recv,
):
    rep, zl = lax.axis_index("rep"), lax.axis_index("fs_0")
    my_y, my_x, core = lax.axis_index("fs_1"), lax.axis_index("fs_2"), lax.axis_index("tp")
    z = rep * 2 + zl

    def device(z_, y_, x_, c_):
        return (z_ // 2, z_ % 2, y_, x_, c_)

    z_plus, z_minus = (z + 1) % 4, (z + 3) % 4
    above, below = device(z_plus, my_y, my_x, core), device(z_minus, my_y, my_x, core)
    sibling = device(z, my_y, my_x, 1 - core)
    z_to = (z + 3 + 2 * core) % 4
    z_from = (z + 1 + 2 * core) % 4
    helper, helped = device(z_to, my_y, my_x, core), device(z_from, my_y, my_x, core)
    x_plus, x_minus = device(z, my_y, (my_x + 1) % 4, core), device(z, my_y, (my_x + 3) % 4, core)
    y_plus, y_minus = device(z, (my_y + 1) % 4, my_x, core), device(z, (my_y + 3) % 4, my_x, core)

    def remote(src, dst, send_sem, recv_sem, target):
        return pltpu.make_async_remote_copy(
            src_ref=src, dst_ref=dst, send_sem=send_sem, recv_sem=recv_sem, device_id=target, device_id_type=MESH
        )

    weights = (wp, wu, wd)
    given = (gp, gu, gd)
    own_row = (zl * 4 + my_y, my_x)
    other_row = ((1 - zl) * 4 + my_y, my_x)

    def stage(which, width):
        return pd.at[pl.ds(pl.multiple_of(which * ROWS, ROWS), ROWS), pl.ds(0, width)]

    def load(which):
        if which < 4:
            source = (wo_in, wi_in, wv_in, wm_in)[which]
        else:
            source = (wu_in, wd_in)[which // 2 - 2].at[:, pl.ds(which % 2 * HID, HID)]
        return pltpu.make_async_copy(source, stage(which, 2 * CH if which < 4 else HID), s_in.at[max(which // 2 - 1, 0)])

    def loaded(t):
        part = pd.at[(pl.ds(0, 4 * ROWS), pl.ds(0, 2 * CH))] if t == MIXER else pd.at[pl.ds(2 * ROWS, 2 * ROWS), pl.ds(0, HID)]
        pltpu.make_async_copy(part, part, s_in.at[t]).wait()

    def cast(t):
        keep, give = weights[t].at[own_row[0], own_row[1]], given[t]
        if t == MIXER:
            loaded(t)
            pieces = [(i, c0, at + i * width, width) for width, c0, at in ((256, 0, 0), (128, 256, 768)) for i in range(3)]
            for i, c0, at, width in pieces + [(3, 0, 3 * CH, CH)]:
                kept = pl.ds(pl.multiple_of(zl * CH + c0, 128), width)
                passed = pl.ds(pl.multiple_of((1 - zl) * CH + c0, 128), width)
                keep[:, at:at + width] = pd[i * ROWS:(i + 1) * ROWS, kept].astype(BF16)
                give[:, at:at + width] = pd[i * ROWS:(i + 1) * ROWS, passed].astype(BF16)
        else:
            first = 2 + 2 * t
            loaded(t)
            keep[...] = stage(first + zl, HID)[...].astype(BF16)
            give[...] = stage(first + 1 - zl, HID)[...].astype(BF16)

    SHIFT = (0, 3, 1, 2)
    HALF = ROWS // 2
    mine, theirs = zl, 1 - zl

    def block(color, k1, k2):
        y_ = (my_y + SHIFT[k1] * color + SHIFT[k2] * (1 - color)) % 4
        x_ = (my_x + SHIFT[k1] * (1 - color) + SHIFT[k2] * color) % 4
        return (color * 4 + y_, x_)

    def ring(color, leg, step):
        along_y = color if leg == 1 else 1 - color
        return device(z, (my_y + step * along_y) % 4, (my_x + step * (1 - along_y)) % 4, core)

    def wcopy(t, color, slot, row, start, rows, target, sent=0):
        part = weights[t].at[row[0], row[1], pl.ds(start, rows)]
        return remote(part, part, sw_send.at[t, sent], sw_recv.at[t, color, slot], target)

    def arrive(t, color, slot, blocks):
        part = weights[t].at[0, pl.ds(0, blocks)]
        remote(part, part, sw_send.at[t, 0], sw_recv.at[t, color, slot], x_plus).wait_recv()

    def first_leg(t, color):
        row = block(color, 0, 0)
        wcopy(t, color, 0, row, 0, ROWS, ring(color, 1, 1), 1).start()
        wcopy(t, color, 0, row, 0, ROWS, ring(color, 1, 3)).start()

    def second_leg(t, color, k):
        row = block(color, k, 0)
        wcopy(t, color, 2 + k, row, 0, ROWS, ring(color, 2, 1)).start()
        wcopy(t, color, 2 + k, row, 0, ROWS, ring(color, 2, 3)).start()

    def zcopy(t, half, row, target):
        return remote(
            given[t].at[pl.ds(half * HALF, HALF)], weights[t].at[row[0], row[1], pl.ds(half * HALF, HALF)],
            sz_send.at[t], sz_recv.at[t], target,
        )

    def start_z(t):
        zcopy(t, 0, own_row, above).start()
        zcopy(t, 1, own_row, below).start()

    def z_arrived(t):
        part = weights[t].at[other_row[0], other_row[1]]
        remote(part, part, sz_send.at[t], sz_recv.at[t], above).wait_recv()

    def g1(t, color):
        arrive(t, color, 0, 2)
        wcopy(t, color, 1, block(color, 1, 0), 0, HALF, ring(color, 1, 1)).start()
        wcopy(t, color, 1, block(color, 2, 0), HALF, HALF, ring(color, 1, 3)).start()

    def g2(t, color):
        arrive(t, color, 1, 1)

    def g3(t, color, k):
        arrive(t, color, 2 + k, 2)
        wcopy(t, color, 6, block(color, k, 1), 0, HALF, ring(color, 2, 1)).start()
        wcopy(t, color, 6, block(color, k, 2), HALF, HALF, ring(color, 2, 3)).start()

    def g4(t):
        for color in (mine, theirs):
            arrive(t, color, 6, 4)

    def chunk(color, k):
        return ((my_y, my_x)[color] + SHIFT[k]) % 4

    def chunk_rows(ref, color, at):
        return ref.at[at] if color == 0 else ref.at[pl.ds(4, 4), at]

    def mix_swap(k, color):
        source = chunk_rows(wp, color, chunk(color, k)).at[:, :, pl.ds(3 * CH, CH)]
        return remote(
            source, chunk_rows(wm2, color, chunk(color, k)), sq_send, sq_recv, (above, below)[color]
        )

    def seq(s):
        return pl.ds(s * SEQ, SEQ)

    def tok_z(s):
        return remote(x.at[0, :, seq(s)], x.at[2, :, seq(s)], sx_send, sx_recv.at[1 + s], helper)

    def tok_sibling():
        return remote(x.at[0], x.at[1], sx_send, sx_recv.at[0], sibling)

    def tok_relay(s):
        return remote(x.at[2, :, seq(s)], x.at[3, :, seq(s)], sx_send, sx_recv.at[4], sibling)

    def first_copy(kind, s):
        source, target, to = ((0, 1, sibling), (0, 2, helper), (2, 3, sibling))[kind]
        return remote(f.at[source, seq(s)], f.at[target, seq(s)], sf_send, sf_recv.at[(0, 1 + s, 4 + s)[kind]], to)

    def mixed_copy(i):
        return remote(mixed.at[2 + i], mixed2.at[i], sm_send, sm_recv, (helped, helper)[i])

    def mix_copy(s):
        rows = (0, slice(None), seq(s))
        return remote(d_send.at[rows], d_recv.at[rows], sd_send.at[0], sd_recv.at[s], sibling)

    def piece(k, color, s):
        return color * 4 + chunk(color, k), pl.ds(0, TOK) if s is None else seq(s)

    def part_copy(slot, k, color, s=None):
        j, rows = piece(k, color, s)
        at = 3 if slot == 0 else 4 + 3 * k + s if k < 2 else 8 + k
        return remote(d_send.at[slot, j, rows], d_recv.at[slot, j, rows], sd_send.at[1], sd_recv.at[at], sibling)

    def sum_copy(k, color, s=None):
        j, rows = piece(k, color, s)
        return remote(z_send.at[j, rows], z_recv.at[j, rows], sr_send, sr_recv.at[0 if k < 3 else 1 + s], helped)

    def came(ref, sem):
        remote(ref, ref, sr_send, sem, x_plus).wait_recv()

    def relay_tokens(s):
        tok_z(s).wait_recv()
        tok_relay(s).start()

    def all_sent(ref, sem):
        remote(ref, ref, sem, sr_recv.at[0], x_plus).wait_send()

    row_id = lax.broadcasted_iota(jnp.int32, (SEQ, 1), 0)

    low = lax.broadcasted_iota(jnp.int32, (1, 128), 1) < 64

    def spread_tokens():
        for j in range(4):
            x[0, j] = own[:, j * COLS:(j + 1) * COLS]
        for x_ in range(4):
            for q in (0, 1):
                a, b = (
                    own[:, pl.ds(1024 + y_ * COLS + (x_ // 2) * 128, 128)].astype(F32) for y_ in (2 * q, 2 * q + 1)
                )
                if x_ % 2 == 0:
                    joined = jnp.where(low, a, pltpu.roll(b, 64, 1))
                else:
                    joined = jnp.where(low, pltpu.roll(a, 64, 1), b)
                x[0, 4 + x_, :, q * 128:(q + 1) * 128] = joined.astype(BF16)

    def project(p, k):
        rows = pl.ds(p * 2 * TOK, 2 * TOK)
        j0, j1 = chunk(0, k), chunk(1, k)
        for a, b in ((0, 768), (768, 1152)):
            total = jnp.dot(
                x[2 * p:2 * p + 2, j0].reshape(2 * TOK, COLS), wp[j0, :, :, a:b].reshape(COLS, b - a),
                preferred_element_type=F32,
            ) + jnp.dot(
                x[2 * p:2 * p + 2, 4 + j1].reshape(2 * TOK, COLS), wp[4:8, j1, :, a:b].reshape(COLS, b - a),
                preferred_element_type=F32,
            )
            if k == 0:
                pd[rows, a:b] = total
            else:
                pd[rows, a:b] += total

    def convolve(g):
        for ch, c0, at in ((256, 0, 0), (128, 256, 768)):
            tap = [taps[k:k + 1, pl.ds(pl.multiple_of(zl * CH + c0, 128), ch)] for k in range(3)]
            for s in range(NSEQ):
                rows = pl.ds(g * TOK + s * SEQ, SEQ)
                product = pd[rows, pl.ds(at + ch, ch)] * pd[rows, pl.ds(at + 2 * ch, ch)]
                before = jnp.where(row_id > 0, pltpu.roll(product, 1, 0), 0.0)
                after = jnp.where(row_id < SEQ - 1, pltpu.roll(product, SEQ - 1, 0), 0.0)
                conv = tap[0] * before + tap[1] * product + tap[2] * after
                mixed[g, seq(s), c0:c0 + ch] = (pd[rows, pl.ds(at, ch)] * conv).astype(BF16)

    def dot_t(rows, w):
        return lax.dot_general(
            rows, w.reshape(COLS, w.shape[-1]), (((1,), (1,)), ((), ())), preferred_element_type=F32
        )

    def mix_sums(s):
        rows = seq(s)
        left, right = mixed[0:2, rows, :].reshape(2 * SEQ, CH), mixed2[0:2, rows, :].reshape(2 * SEQ, CH)
        for j in range(NCOL):
            total = dot_t(left, wp[j, :, :, 3 * CH:4 * CH]) + dot_t(right, wm2[j])
            acc[j, rows, :] = total[:SEQ]
            d_send[0, j, rows, :] = total[SEQ:].astype(BF16)
        mix_copy(s).start()

    def ffn_sums(p, k, s=None):
        rows = pl.ds(0, TOK) if s is None else seq(s)
        half = TOK if s is None else SEQ
        for color in (0, 1):
            j = color * 4 + chunk(color, k)
            w = wd[j] if color == 0 else wd[4:8, j - 4]
            total = dot_t(hid[2 * p:2 * p + 2, rows, :].reshape(2 * half, HID), w)
            d_send[p, j, rows, :] = total[half:].astype(BF16)
            if p == 0:
                acc[j, rows, :] = total[:half]
            else:
                held[k % 2, color, rows, :] = total[:half]
        for color in (0, 1):
            part_copy(p, k, color, s).start()

    def ffn_send(k, s=None):
        if k < 3:
            rows = pl.ds(0, TOK) if s is None else seq(s)
            came(d_recv.at[1, pl.ds(0, 2), rows], sd_recv.at[4 + 3 * k + s if k < 2 else 8 + k])
        for color in (0, 1):
            j, rows = piece(k, color, s)
            z_send[j, rows, :] = (held[k % 2, color, rows, :] + d_recv[1, j, rows, :].astype(F32)).astype(BF16)
        for color in (0, 1):
            sum_copy(k, color, s).start()

    def natural(parts):
        tiles = [[parts[4 + x_][:, q * 128:(q + 1) * 128] for q in (0, 1)] for x_ in range(4)]
        result = list(parts[:4])
        for y_ in range(4):
            for p in (0, 1):
                a, b = tiles[2 * p][y_ // 2], tiles[2 * p + 1][y_ // 2]
                if y_ % 2 == 0:
                    result.append(jnp.where(low, a, pltpu.roll(b, 64, 1)))
                else:
                    result.append(jnp.where(low, pltpu.roll(a, 64, 1), b))
        return jnp.concatenate(result, axis=1)

    def normed(base, arrived, gain, s, target):
        step_rows = 32

        def step(i, _):
            rows = pl.ds(pl.multiple_of(s * SEQ + i * step_rows, step_rows), step_rows)
            v = SCALE * base[rows, :].astype(F32) + arrived(rows)
            center = v - jnp.mean(v, axis=-1, keepdims=True)
            spread = jnp.mean(center * center, axis=-1, keepdims=True)
            target[rows, :] = (center * lax.rsqrt(spread + EPS) * gain[...]).astype(BF16)
            return 0

        lax.fori_loop(0, SEQ // step_rows, step, 0)

    def expand(g, s=None):
        rows = pl.ds(0, TOK) if s is None else seq(s)

        def step(j, _):
            cols = pl.ds(pl.multiple_of(j * 512, 512), 512)
            raised = jnp.maximum(jnp.dot(f[g, rows, :], wu[:, :, :, cols].reshape(D, 512), preferred_element_type=F32), 0.0)
            hid[g, rows, cols] = (raised * raised).astype(BF16)
            return 0

        lax.fori_loop(0, HID // 512, step, 0)

    barrier = pltpu.get_barrier_semaphore()
    for other in (x_plus, x_minus, y_plus, y_minus, above, below, sibling):
        pl.semaphore_signal(barrier, inc=1, device_id=other, device_id_type=MESH)
    own_tokens = pltpu.make_async_copy(tok, own, sx_own)
    for which in range(4):
        load(which).start()
    own_tokens.start()
    for which in range(4, 8):
        load(which).start()

    def small_loads(wait):
        for i, (source, target) in enumerate(((taps_in, taps), (gain1_in, gain1), (gain2_in, gain2))):
            copy = pltpu.make_async_copy(source, target, s_small.at[i])
            copy.wait() if wait else copy.start()

    small_loads(False)
    cast(MIXER)
    pl.semaphore_wait(barrier, 7)

    both = (mine, theirs)

    def each(step, t, *rest):
        for color in both:
            step(t, color, *rest)

    start_z(MIXER)
    first_leg(MIXER, mine)
    second_leg(MIXER, mine, 0)
    own_tokens.wait()
    spread_tokens()
    tok_z(0).start()
    tok_sibling().start()
    cast(UP)
    start_z(UP)
    tok_z(1).start()
    tok_z(2).start()
    cast(DOWN)
    start_z(DOWN)
    small_loads(True)
    z_arrived(MIXER)
    first_leg(MIXER, theirs)
    second_leg(MIXER, theirs, 0)
    g1(MIXER, mine)
    second_leg(MIXER, mine, 1)
    relay_tokens(0)
    g1(MIXER, theirs)
    second_leg(MIXER, mine, 2)
    second_leg(MIXER, theirs, 1)
    second_leg(MIXER, theirs, 2)
    g2(MIXER, mine)
    second_leg(MIXER, mine, 3)
    g2(MIXER, theirs)
    second_leg(MIXER, theirs, 3)
    for color in (0, 1):
        mix_swap(0, color).start()
    each(g3, MIXER, 0)
    relay_tokens(1)
    tok_sibling().wait_recv()
    project(0, 0)
    each(g3, MIXER, 1)
    relay_tokens(2)
    each(g3, MIXER, 2)
    came(x.at[3], sx_recv.at[4])
    project(1, 0)
    each(g3, MIXER, 3)
    z_arrived(UP)
    each(first_leg, UP)
    each(second_leg, UP, 0)
    for k in (1, 2):
        for color in (0, 1):
            mix_swap(k, color).start()
    project(1, 1)
    project(1, 2)
    g4(MIXER)
    for color in (0, 1):
        mix_swap(3, color).start()
    project(1, 3)
    convolve(3)
    mixed_copy(1).start()
    convolve(2)
    mixed_copy(0).start()
    each(g1, UP)
    each(second_leg, UP, 1)
    z_arrived(DOWN)
    each(first_leg, DOWN)
    each(second_leg, UP, 2)
    project(0, 1)
    each(g3, UP, 0)
    project(0, 2)
    each(g2, UP)
    each(second_leg, UP, 3)
    project(0, 3)
    convolve(1)
    convolve(0)
    came(wm2, sq_recv)
    came(mixed2, sm_recv)

    def mixing(rows):
        return jnp.concatenate([acc[j, rows, :] + d_recv[0, j, rows, :].astype(F32) for j in range(NCOL)], axis=1)

    def make_first(s):
        mix_copy(s).wait_recv()
        normed(own, mixing, gain1, s, f.at[0])
        first_copy(1, s).start()
        first_copy(0, s).start()

    mix_sums(0)
    each(g3, UP, 1)
    mix_sums(1)
    make_first(0)
    each(g1, DOWN)
    mix_sums(2)
    each(g3, UP, 2)
    make_first(1)
    second_leg(DOWN, mine, 0)
    second_leg(DOWN, theirs, 0)
    make_first(2)
    each(g3, UP, 3)
    for k in (1, 2):
        each(second_leg, DOWN, k)
    each(g2, DOWN)
    each(second_leg, DOWN, 3)
    came(f.at[1], sf_recv.at[0])
    g4(UP)
    expand(0)
    each(g3, DOWN, 0)
    all_sent(d_send.at[0], sd_send.at[0])
    first_copy(1, 0).wait_recv()
    first_copy(2, 0).start()
    expand(2, 0)
    first_copy(2, 0).wait_recv()
    expand(3, 0)
    ffn_sums(1, 0, 0)
    expand(1)
    ffn_send(0, 0)
    each(g3, DOWN, 1)
    first_copy(1, 1).wait_recv()
    first_copy(2, 1).start()
    expand(2, 1)
    each(g3, DOWN, 2)
    first_copy(2, 1).wait_recv()
    expand(3, 1)
    ffn_sums(1, 0, 1)
    each(g3, DOWN, 3)
    ffn_sums(1, 1, 0)
    ffn_send(0, 1)
    ffn_sums(1, 1, 1)
    ffn_send(1, 0)
    first_copy(1, 2).wait_recv()
    first_copy(2, 2).start()
    expand(2, 2)
    ffn_send(1, 1)
    first_copy(2, 2).wait_recv()
    expand(3, 2)
    ffn_sums(1, 0, 2)
    ffn_sums(1, 1, 2)
    ffn_send(0, 2)
    ffn_sums(1, 2)
    ffn_send(1, 2)
    g4(DOWN)
    ffn_sums(1, 3)
    ffn_send(2)
    ffn_sums(0, 0)
    came(d_recv.at[1, pl.ds(0, 2)], sd_recv.at[11])
    for s in range(NSEQ):
        ffn_send(3, s)
    for k in (1, 2, 3):
        ffn_sums(0, k)
    came(d_recv.at[0], sd_recv.at[3])
    came(z_recv.at[pl.ds(0, 6)], sr_recv.at[0])

    def lowered(rows):
        return natural([
            acc[j, rows, :] + d_recv[0, j, rows, :].astype(F32) + z_recv[j, rows, :].astype(F32) for j in range(NCOL)
        ])

    for s in range(NSEQ):
        came(z_recv.at[pl.ds(0, 2), seq(s)], sr_recv.at[1 + s])
        normed(f.at[0], lowered, gain2, s, own)

    for t in range(3):
        all_sent(weights[t].at[pl.ds(0, 7)], sw_send.at[t, 0])
        all_sent(weights[t].at[0, pl.ds(0, 2)], sw_send.at[t, 1])
        all_sent(given[t], sz_send.at[t])
    all_sent(x.at[pl.ds(0, 3)], sx_send)
    all_sent(f.at[pl.ds(0, 3)], sf_send)
    all_sent(wm2, sq_send)
    all_sent(mixed2, sm_send)
    all_sent(d_send, sd_send.at[1])
    all_sent(z_send, sr_send)


def local(tokens, outer_weight, inner_weight, value_weight, conv_taps, mix_out, norm_first, up_weight, down_weight, norm_second):
    hbm = pl.BlockSpec(memory_space=pl.ANY)
    vmem = pl.BlockSpec(memory_space=pltpu.VMEM)
    dma = pltpu.SemaphoreType.DMA
    return pl.pallas_call(
        kernel,
        name="mixer_ffn",
        out_shape=pltpu.VMEM((TOK, D), BF16),
        in_specs=[hbm] * 10,
        out_specs=vmem,
        scratch_shapes=[pltpu.VMEM((8, 4, ROWS, w), BF16) for w in WIDTHS]
        + [pltpu.VMEM((8, 4, ROWS, CH), BF16)]
        + [pltpu.VMEM((ROWS, w), BF16) for w in WIDTHS]
        + [
            pltpu.VMEM((4, 8, TOK, COLS), BF16),
            pltpu.VMEM((4, TOK, D), BF16),
            pltpu.VMEM((4, TOK, CH), BF16),
            pltpu.VMEM((2, TOK, CH), BF16),
            pltpu.VMEM((4, TOK, HID), BF16),
            pltpu.VMEM((4 * TOK, 3 * CH), F32),
            pltpu.VMEM((2, NCOL, TOK, COLS), BF16),
            pltpu.VMEM((2, NCOL, TOK, COLS), BF16),
            pltpu.VMEM((NCOL, TOK, COLS), BF16),
            pltpu.VMEM((NCOL, TOK, COLS), BF16),
            pltpu.VMEM((NCOL, TOK, COLS), F32),
            pltpu.VMEM((2, 2, TOK, COLS), F32),
            pltpu.VMEM((3, 2 * CH), F32),
            pltpu.VMEM((1, D), F32),
            pltpu.VMEM((1, D), F32),
            dma((3,)),
            dma((3,)),
            dma((3, 2)),
            dma((3, 2, 7)),
            dma((3,)),
            dma((3,)),
            dma,
            dma,
            dma((5,)),
            dma,
            dma((7,)),
            dma,
            dma,
            dma,
            dma,
            dma((2,)),
            dma((12,)),
            dma,
            dma((4,)),
        ],
        compiler_params=pltpu.CompilerParams(
            collective_id=0, has_side_effects=True, vmem_limit_bytes=62 * 1024 * 1024
        ),
    )(
        tokens, outer_weight, inner_weight, value_weight, mix_out.T, up_weight, down_weight.T,
        conv_taps, norm_first.reshape(1, D), norm_second.reshape(1, D),
    )


def solution(mesh):
    finer = Mesh(
        mesh.devices.reshape(mesh.shape["rep"], 2, 4, 4, mesh.shape["tp"]),
        ("rep", "fs_0", "fs_1", "fs_2", "tp"),
    )
    placed = (
        P(REP_FS_TP, None),
        P(FS, "tp"),
        P(FS, "tp"),
        P(FS, "tp"),
        P(None, "tp"),
        P("tp", FS),
        P(),
        P(FS, "tp"),
        P("tp", FS),
        P(),
    )
    return jax.shard_map(
        local, mesh=finer, in_specs=placed, out_specs=P(REP_FS_TP, None), check_vma=False
    )
```

```python
import jax
import jax.numpy as jnp
from jax import lax
from jax.experimental import pallas as pl
from jax.experimental.pallas import tpu as pltpu
from jax.sharding import Mesh
from jax.sharding import PartitionSpec as P

SEQ = 128
FS = ("fs_0", "fs_1", "fs_2")
REP_FS_TP = ("rep", "fs_0", "fs_1", "fs_2", "tp")
MESH = pl.DeviceIdType.MESH
SCALE = 2.0**0.25
EPS = 1e-05
F32 = jnp.float32
BF16 = jnp.bfloat16

D = 2048
ROWS = 64
TOK = 384
CH = 384
HID = 1024
NSEQ = TOK // SEQ
WIDTHS = (4 * CH, HID, HID)
MIXER, UP, DOWN = range(3)
COLS = 256
NCOL = D // COLS


def kernel(
    tok, wo_in, wi_in, wv_in, wm_in, wu_in, wd_in, taps_in, gain1_in, gain2_in, own,
    wp, wu, wd, wm2, gp, gu, gd,
    x, f, mixed, mixed2, hid, pd, d_send, d_recv, z_send, z_recv, acc, held, taps, gain1, gain2,
    s_small, s_in, sw_send, sw_recv, sz_send, sz_recv, sx_own, sx_send, sx_recv, sf_send, sf_recv,
    sq_send, sq_recv, sm_send, sm_recv, sd_send, sd_recv, sr_send, sr_recv,
):
    rep, zl = lax.axis_index("rep"), lax.axis_index("fs_0")
    my_y, my_x, core = lax.axis_index("fs_1"), lax.axis_index("fs_2"), lax.axis_index("tp")
    z = rep * 2 + zl

    def device(z_, y_, x_, c_):
        return (z_ // 2, z_ % 2, y_, x_, c_)

    z_plus, z_minus = (z + 1) % 4, (z + 3) % 4
    above, below = device(z_plus, my_y, my_x, core), device(z_minus, my_y, my_x, core)
    sibling = device(z, my_y, my_x, 1 - core)
    z_to = (z + 3 + 2 * core) % 4
    z_from = (z + 1 + 2 * core) % 4
    helper, helped = device(z_to, my_y, my_x, core), device(z_from, my_y, my_x, core)
    x_plus, x_minus = device(z, my_y, (my_x + 1) % 4, core), device(z, my_y, (my_x + 3) % 4, core)
    y_plus, y_minus = device(z, (my_y + 1) % 4, my_x, core), device(z, (my_y + 3) % 4, my_x, core)

    def remote(src, dst, send_sem, recv_sem, target):
        return pltpu.make_async_remote_copy(
            src_ref=src, dst_ref=dst, send_sem=send_sem, recv_sem=recv_sem, device_id=target, device_id_type=MESH
        )

    weights = (wp, wu, wd)
    given = (gp, gu, gd)
    own_row = (zl * 4 + my_y, my_x)
    other_row = ((1 - zl) * 4 + my_y, my_x)

    def stage(which, width):
        return pd.at[pl.ds(pl.multiple_of(which * ROWS, ROWS), ROWS), pl.ds(0, width)]

    def load(which):
        if which < 4:
            source = (wo_in, wi_in, wv_in, wm_in)[which]
        else:
            source = (wu_in, wd_in)[which // 2 - 2].at[:, pl.ds(which % 2 * HID, HID)]
        return pltpu.make_async_copy(source, stage(which, 2 * CH if which < 4 else HID), s_in.at[max(which // 2 - 1, 0)])

    def loaded(t):
        part = pd.at[(pl.ds(0, 4 * ROWS), pl.ds(0, 2 * CH))] if t == MIXER else pd.at[pl.ds(2 * ROWS, 2 * ROWS), pl.ds(0, HID)]
        pltpu.make_async_copy(part, part, s_in.at[t]).wait()

    def cast(t):
        keep, give = weights[t].at[own_row[0], own_row[1]], given[t]
        if t == MIXER:
            loaded(t)
            pieces = [(i, c0, at + i * width, width) for width, c0, at in ((256, 0, 0), (128, 256, 768)) for i in range(3)]
            for i, c0, at, width in pieces + [(3, 0, 3 * CH, CH)]:
                kept = pl.ds(pl.multiple_of(zl * CH + c0, 128), width)
                passed = pl.ds(pl.multiple_of((1 - zl) * CH + c0, 128), width)
                keep[:, at:at + width] = pd[i * ROWS:(i + 1) * ROWS, kept].astype(BF16)
                give[:, at:at + width] = pd[i * ROWS:(i + 1) * ROWS, passed].astype(BF16)
        else:
            first = 2 + 2 * t
            loaded(t)
            keep[...] = stage(first + zl, HID)[...].astype(BF16)
            give[...] = stage(first + 1 - zl, HID)[...].astype(BF16)

    SHIFT = (0, 3, 1, 2)
    HALF = ROWS // 2
    mine, theirs = zl, 1 - zl

    def block(color, k1, k2):
        y_ = (my_y + SHIFT[k1] * color + SHIFT[k2] * (1 - color)) % 4
        x_ = (my_x + SHIFT[k1] * (1 - color) + SHIFT[k2] * color) % 4
        return (color * 4 + y_, x_)

    def ring(color, leg, step):
        along_y = color if leg == 1 else 1 - color
        return device(z, (my_y + step * along_y) % 4, (my_x + step * (1 - along_y)) % 4, core)

    def wcopy(t, color, slot, row, start, rows, target, sent=0):
        part = weights[t].at[row[0], row[1], pl.ds(start, rows)]
        return remote(part, part, sw_send.at[t, sent], sw_recv.at[t, color, slot], target)

    def arrive(t, color, slot, blocks):
        part = weights[t].at[0, pl.ds(0, blocks)]
        remote(part, part, sw_send.at[t, 0], sw_recv.at[t, color, slot], x_plus).wait_recv()

    def first_leg(t, color):
        row = block(color, 0, 0)
        wcopy(t, color, 0, row, 0, ROWS, ring(color, 1, 1), 1).start()
        wcopy(t, color, 0, row, 0, ROWS, ring(color, 1, 3)).start()

    def second_leg(t, color, k):
        row = block(color, k, 0)
        wcopy(t, color, 2 + k, row, 0, ROWS, ring(color, 2, 1)).start()
        wcopy(t, color, 2 + k, row, 0, ROWS, ring(color, 2, 3)).start()

    def zcopy(t, half, row, target):
        return remote(
            given[t].at[pl.ds(half * HALF, HALF)], weights[t].at[row[0], row[1], pl.ds(half * HALF, HALF)],
            sz_send.at[t], sz_recv.at[t], target,
        )

    def start_z(t):
        zcopy(t, 0, own_row, above).start()
        zcopy(t, 1, own_row, below).start()

    def z_arrived(t):
        part = weights[t].at[other_row[0], other_row[1]]
        remote(part, part, sz_send.at[t], sz_recv.at[t], above).wait_recv()

    def g1(t, color):
        arrive(t, color, 0, 2)
        wcopy(t, color, 1, block(color, 1, 0), 0, HALF, ring(color, 1, 1)).start()
        wcopy(t, color, 1, block(color, 2, 0), HALF, HALF, ring(color, 1, 3)).start()

    def g2(t, color):
        arrive(t, color, 1, 1)

    def g3(t, color, k):
        arrive(t, color, 2 + k, 2)
        wcopy(t, color, 6, block(color, k, 1), 0, HALF, ring(color, 2, 1)).start()
        wcopy(t, color, 6, block(color, k, 2), HALF, HALF, ring(color, 2, 3)).start()

    def g4(t):
        for color in (mine, theirs):
            arrive(t, color, 6, 4)

    def chunk(color, k):
        return ((my_y, my_x)[color] + SHIFT[k]) % 4

    def chunk_rows(ref, color, at):
        return ref.at[at] if color == 0 else ref.at[pl.ds(4, 4), at]

    def mix_swap(k, color):
        source = chunk_rows(wp, color, chunk(color, k)).at[:, :, pl.ds(3 * CH, CH)]
        return remote(
            source, chunk_rows(wm2, color, chunk(color, k)), sq_send, sq_recv, (above, below)[color]
        )

    def seq(s):
        return pl.ds(s * SEQ, SEQ)

    def tok_z(s):
        return remote(x.at[0, :, seq(s)], x.at[2, :, seq(s)], sx_send, sx_recv.at[1 + s], helper)

    def tok_sibling():
        return remote(x.at[0], x.at[1], sx_send, sx_recv.at[0], sibling)

    def tok_relay(s):
        return remote(x.at[2, :, seq(s)], x.at[3, :, seq(s)], sx_send, sx_recv.at[4], sibling)

    def first_copy(kind, s):
        source, target, to = ((0, 1, sibling), (0, 2, helper), (2, 3, sibling))[kind]
        return remote(f.at[source, seq(s)], f.at[target, seq(s)], sf_send, sf_recv.at[(0, 1 + s, 4 + s)[kind]], to)

    def mixed_copy(i):
        return remote(mixed.at[2 + i], mixed2.at[i], sm_send, sm_recv, (helped, helper)[i])

    def mix_copy(s):
        rows = (0, slice(None), seq(s))
        return remote(d_send.at[rows], d_recv.at[rows], sd_send.at[0], sd_recv.at[s], sibling)

    def piece(k, color, s):
        return color * 4 + chunk(color, k), pl.ds(0, TOK) if s is None else seq(s)

    def part_copy(slot, k, color, s=None):
        j, rows = piece(k, color, s)
        at = 3 if slot == 0 else 4 + 3 * k + s if k < 2 else 8 + k
        return remote(d_send.at[slot, j, rows], d_recv.at[slot, j, rows], sd_send.at[1], sd_recv.at[at], sibling)

    def sum_copy(k, color, s=None):
        j, rows = piece(k, color, s)
        return remote(z_send.at[j, rows], z_recv.at[j, rows], sr_send, sr_recv.at[0 if k < 3 else 1 + s], helped)

    def came(ref, sem):
        remote(ref, ref, sr_send, sem, x_plus).wait_recv()

    def relay_tokens(s):
        tok_z(s).wait_recv()
        tok_relay(s).start()

    def all_sent(ref, sem):
        remote(ref, ref, sem, sr_recv.at[0], x_plus).wait_send()

    row_id = lax.broadcasted_iota(jnp.int32, (SEQ, 1), 0)

    low = lax.broadcasted_iota(jnp.int32, (1, 128), 1) < 64

    def spread_tokens():
        for j in range(4):
            x[0, j] = own[:, j * COLS:(j + 1) * COLS]
        for x_ in range(4):
            for q in (0, 1):
                a, b = (
                    own[:, pl.ds(1024 + y_ * COLS + (x_ // 2) * 128, 128)].astype(F32) for y_ in (2 * q, 2 * q + 1)
                )
                if x_ % 2 == 0:
                    joined = jnp.where(low, a, pltpu.roll(b, 64, 1))
                else:
                    joined = jnp.where(low, pltpu.roll(a, 64, 1), b)
                x[0, 4 + x_, :, q * 128:(q + 1) * 128] = joined.astype(BF16)

    def project(p, k):
        rows = pl.ds(p * 2 * TOK, 2 * TOK)
        j0, j1 = chunk(0, k), chunk(1, k)
        for a, b in ((0, 768), (768, 1152)):
            total = jnp.dot(
                x[2 * p:2 * p + 2, j0].reshape(2 * TOK, COLS), wp[j0, :, :, a:b].reshape(COLS, b - a),
                preferred_element_type=F32,
            ) + jnp.dot(
                x[2 * p:2 * p + 2, 4 + j1].reshape(2 * TOK, COLS), wp[4:8, j1, :, a:b].reshape(COLS, b - a),
                preferred_element_type=F32,
            )
            if k == 0:
                pd[rows, a:b] = total
            else:
                pd[rows, a:b] += total

    def convolve(g):
        for ch, c0, at in ((256, 0, 0), (128, 256, 768)):
            tap = [taps[k:k + 1, pl.ds(pl.multiple_of(zl * CH + c0, 128), ch)] for k in range(3)]
            for s in range(NSEQ):
                rows = pl.ds(g * TOK + s * SEQ, SEQ)
                product = pd[rows, pl.ds(at + ch, ch)] * pd[rows, pl.ds(at + 2 * ch, ch)]
                before = jnp.where(row_id > 0, pltpu.roll(product, 1, 0), 0.0)
                after = jnp.where(row_id < SEQ - 1, pltpu.roll(product, SEQ - 1, 0), 0.0)
                conv = tap[0] * before + tap[1] * product + tap[2] * after
                mixed[g, seq(s), c0:c0 + ch] = (pd[rows, pl.ds(at, ch)] * conv).astype(BF16)

    def dot_t(rows, w):
        return lax.dot_general(
            rows, w.reshape(COLS, w.shape[-1]), (((1,), (1,)), ((), ())), preferred_element_type=F32
        )

    def mix_sums(s):
        rows = seq(s)
        left, right = mixed[0:2, rows, :].reshape(2 * SEQ, CH), mixed2[0:2, rows, :].reshape(2 * SEQ, CH)
        for j in range(NCOL):
            total = dot_t(left, wp[j, :, :, 3 * CH:4 * CH]) + dot_t(right, wm2[j])
            acc[j, rows, :] = total[:SEQ]
            d_send[0, j, rows, :] = total[SEQ:].astype(BF16)
        mix_copy(s).start()

    def ffn_sums(p, k, s=None):
        rows = pl.ds(0, TOK) if s is None else seq(s)
        half = TOK if s is None else SEQ
        for color in (0, 1):
            j = color * 4 + chunk(color, k)
            w = wd[j] if color == 0 else wd[4:8, j - 4]
            total = dot_t(hid[2 * p:2 * p + 2, rows, :].reshape(2 * half, HID), w)
            d_send[p, j, rows, :] = total[half:].astype(BF16)
            if p == 0:
                acc[j, rows, :] = total[:half]
            else:
                held[k % 2, color, rows, :] = total[:half]
        for color in (0, 1):
            part_copy(p, k, color, s).start()

    def ffn_send(k, s=None):
        if k < 3:
            rows = pl.ds(0, TOK) if s is None else seq(s)
            came(d_recv.at[1, pl.ds(0, 2), rows], sd_recv.at[4 + 3 * k + s if k < 2 else 8 + k])
        for color in (0, 1):
            j, rows = piece(k, color, s)
            z_send[j, rows, :] = (held[k % 2, color, rows, :] + d_recv[1, j, rows, :].astype(F32)).astype(BF16)
        for color in (0, 1):
            sum_copy(k, color, s).start()

    def natural(parts):
        tiles = [[parts[4 + x_][:, q * 128:(q + 1) * 128] for q in (0, 1)] for x_ in range(4)]
        result = list(parts[:4])
        for y_ in range(4):
            for p in (0, 1):
                a, b = tiles[2 * p][y_ // 2], tiles[2 * p + 1][y_ // 2]
                if y_ % 2 == 0:
                    result.append(jnp.where(low, a, pltpu.roll(b, 64, 1)))
                else:
                    result.append(jnp.where(low, pltpu.roll(a, 64, 1), b))
        return jnp.concatenate(result, axis=1)

    def normed(base, arrived, gain, s, target):
        step_rows = 32

        def step(i, _):
            rows = pl.ds(pl.multiple_of(s * SEQ + i * step_rows, step_rows), step_rows)
            v = SCALE * base[rows, :].astype(F32) + arrived(rows)
            center = v - jnp.mean(v, axis=-1, keepdims=True)
            spread = jnp.mean(center * center, axis=-1, keepdims=True)
            target[rows, :] = (center * lax.rsqrt(spread + EPS) * gain[...]).astype(BF16)
            return 0

        lax.fori_loop(0, SEQ // step_rows, step, 0, unroll=2)

    def expand(g, s=None):
        rows = pl.ds(0, TOK) if s is None else seq(s)

        def step(j, _):
            cols = pl.ds(pl.multiple_of(j * 512, 512), 512)
            raised = jnp.maximum(jnp.dot(f[g, rows, :], wu[:, :, :, cols].reshape(D, 512), preferred_element_type=F32), 0.0)
            hid[g, rows, cols] = (raised * raised).astype(BF16)
            return 0

        lax.fori_loop(0, HID // 512, step, 0)

    barrier = pltpu.get_barrier_semaphore()
    for other in (x_plus, x_minus, y_plus, y_minus, above, below, sibling):
        pl.semaphore_signal(barrier, inc=1, device_id=other, device_id_type=MESH)
    own_tokens = pltpu.make_async_copy(tok, own, sx_own)
    for which in range(4):
        load(which).start()
    own_tokens.start()
    for which in range(4, 8):
        load(which).start()

    def small_loads(wait):
        for i, (source, target) in enumerate(((taps_in, taps), (gain1_in, gain1), (gain2_in, gain2))):
            copy = pltpu.make_async_copy(source, target, s_small.at[i])
            copy.wait() if wait else copy.start()

    small_loads(False)
    cast(MIXER)
    pl.semaphore_wait(barrier, 7)

    both = (mine, theirs)

    def each(step, t, *rest):
        for color in both:
            step(t, color, *rest)

    start_z(MIXER)
    first_leg(MIXER, mine)
    second_leg(MIXER, mine, 0)
    own_tokens.wait()
    spread_tokens()
    tok_z(0).start()
    tok_sibling().start()
    cast(UP)
    start_z(UP)
    tok_z(1).start()
    tok_z(2).start()
    cast(DOWN)
    start_z(DOWN)
    small_loads(True)
    z_arrived(MIXER)
    first_leg(MIXER, theirs)
    second_leg(MIXER, theirs, 0)
    g1(MIXER, mine)
    second_leg(MIXER, mine, 1)
    relay_tokens(0)
    g1(MIXER, theirs)
    second_leg(MIXER, mine, 2)
    second_leg(MIXER, theirs, 1)
    second_leg(MIXER, theirs, 2)
    g2(MIXER, mine)
    second_leg(MIXER, mine, 3)
    g2(MIXER, theirs)
    second_leg(MIXER, theirs, 3)
    for color in (0, 1):
        mix_swap(0, color).start()
    each(g3, MIXER, 0)
    relay_tokens(1)
    tok_sibling().wait_recv()
    project(0, 0)
    each(g3, MIXER, 1)
    relay_tokens(2)
    each(g3, MIXER, 2)
    came(x.at[3], sx_recv.at[4])
    project(1, 0)
    each(g3, MIXER, 3)
    z_arrived(UP)
    each(first_leg, UP)
    each(second_leg, UP, 0)
    for k in (1, 2):
        for color in (0, 1):
            mix_swap(k, color).start()
    project(1, 1)
    project(1, 2)
    g4(MIXER)
    for color in (0, 1):
        mix_swap(3, color).start()
    project(1, 3)
    convolve(3)
    mixed_copy(1).start()
    convolve(2)
    mixed_copy(0).start()
    each(g1, UP)
    each(second_leg, UP, 1)
    z_arrived(DOWN)
    each(first_leg, DOWN)
    each(second_leg, UP, 2)
    project(0, 1)
    each(g3, UP, 0)
    project(0, 2)
    each(g2, UP)
    each(second_leg, UP, 3)
    project(0, 3)
    convolve(1)
    convolve(0)
    came(wm2, sq_recv)
    came(mixed2, sm_recv)

    def mixing(rows):
        return jnp.concatenate([acc[j, rows, :] + d_recv[0, j, rows, :].astype(F32) for j in range(NCOL)], axis=1)

    def make_first(s):
        mix_copy(s).wait_recv()
        normed(own, mixing, gain1, s, f.at[0])
        first_copy(1, s).start()
        first_copy(0, s).start()

    mix_sums(0)
    each(g3, UP, 1)
    mix_sums(1)
    make_first(0)
    each(g1, DOWN)
    mix_sums(2)
    each(g3, UP, 2)
    make_first(1)
    second_leg(DOWN, mine, 0)
    second_leg(DOWN, theirs, 0)
    make_first(2)
    each(g3, UP, 3)
    for k in (1, 2):
        each(second_leg, DOWN, k)
    each(g2, DOWN)
    each(second_leg, DOWN, 3)
    came(f.at[1], sf_recv.at[0])
    first_copy(1, 0).wait_recv()
    first_copy(2, 0).start()
    g4(UP)
    expand(2, 0)
    first_copy(2, 0).wait_recv()
    expand(3, 0)
    ffn_sums(1, 0, 0)
    each(g3, DOWN, 0)
    first_copy(1, 1).wait_recv()
    first_copy(2, 1).start()
    expand(2, 1)
    ffn_send(0, 0)
    each(g3, DOWN, 1)
    expand(0)
    each(g3, DOWN, 2)
    first_copy(2, 1).wait_recv()
    expand(3, 1)
    ffn_sums(1, 0, 1)
    each(g3, DOWN, 3)
    first_copy(1, 2).wait_recv()
    first_copy(2, 2).start()
    ffn_sums(1, 1, 0)
    ffn_send(0, 1)
    ffn_sums(1, 1, 1)
    ffn_send(1, 0)
    expand(2, 2)
    ffn_send(1, 1)
    first_copy(2, 2).wait_recv()
    expand(3, 2)
    ffn_sums(1, 0, 2)
    ffn_sums(1, 1, 2)
    ffn_send(0, 2)
    ffn_sums(1, 2)
    ffn_send(1, 2)
    expand(1)
    ffn_send(2)
    g4(DOWN)
    ffn_sums(1, 3)
    all_sent(d_send.at[0], sd_send.at[0])
    ffn_sums(0, 0)
    came(d_recv.at[1, pl.ds(0, 2)], sd_recv.at[11])
    for s in range(NSEQ):
        ffn_send(3, s)
    for k in (1, 2, 3):
        ffn_sums(0, k)
    came(d_recv.at[0], sd_recv.at[3])
    came(z_recv.at[pl.ds(0, 6)], sr_recv.at[0])

    def lowered(rows):
        return natural([
            acc[j, rows, :] + d_recv[0, j, rows, :].astype(F32) + z_recv[j, rows, :].astype(F32) for j in range(NCOL)
        ])

    for s in range(NSEQ):
        came(z_recv.at[pl.ds(0, 2), seq(s)], sr_recv.at[1 + s])
        normed(f.at[0], lowered, gain2, s, own)

    for t in range(3):
        all_sent(weights[t].at[pl.ds(0, 7)], sw_send.at[t, 0])
        all_sent(weights[t].at[0, pl.ds(0, 2)], sw_send.at[t, 1])
        all_sent(given[t], sz_send.at[t])
    all_sent(x.at[pl.ds(0, 3)], sx_send)
    all_sent(f.at[pl.ds(0, 3)], sf_send)
    all_sent(wm2, sq_send)
    all_sent(mixed2, sm_send)
    all_sent(d_send, sd_send.at[1])
    all_sent(z_send, sr_send)


def local(tokens, outer_weight, inner_weight, value_weight, conv_taps, mix_out, norm_first, up_weight, down_weight, norm_second):
    hbm = pl.BlockSpec(memory_space=pl.ANY)
    vmem = pl.BlockSpec(memory_space=pltpu.VMEM)
    dma = pltpu.SemaphoreType.DMA
    return pl.pallas_call(
        kernel,
        name="mixer_ffn",
        out_shape=pltpu.VMEM((TOK, D), BF16),
        in_specs=[hbm] * 10,
        out_specs=vmem,
        scratch_shapes=[pltpu.VMEM((8, 4, ROWS, w), BF16) for w in WIDTHS]
        + [pltpu.VMEM((8, 4, ROWS, CH), BF16)]
        + [pltpu.VMEM((ROWS, w), BF16) for w in WIDTHS]
        + [
            pltpu.VMEM((4, 8, TOK, COLS), BF16),
            pltpu.VMEM((4, TOK, D), BF16),
            pltpu.VMEM((4, TOK, CH), BF16),
            pltpu.VMEM((2, TOK, CH), BF16),
            pltpu.VMEM((4, TOK, HID), BF16),
            pltpu.VMEM((4 * TOK, 3 * CH), F32),
            pltpu.VMEM((2, NCOL, TOK, COLS), BF16),
            pltpu.VMEM((2, NCOL, TOK, COLS), BF16),
            pltpu.VMEM((NCOL, TOK, COLS), BF16),
            pltpu.VMEM((NCOL, TOK, COLS), BF16),
            pltpu.VMEM((NCOL, TOK, COLS), F32),
            pltpu.VMEM((2, 2, TOK, COLS), F32),
            pltpu.VMEM((3, 2 * CH), F32),
            pltpu.VMEM((1, D), F32),
            pltpu.VMEM((1, D), F32),
            dma((3,)),
            dma((3,)),
            dma((3, 2)),
            dma((3, 2, 7)),
            dma((3,)),
            dma((3,)),
            dma,
            dma,
            dma((5,)),
            dma,
            dma((7,)),
            dma,
            dma,
            dma,
            dma,
            dma((2,)),
            dma((12,)),
            dma,
            dma((4,)),
        ],
        compiler_params=pltpu.CompilerParams(
            collective_id=0, has_side_effects=True, vmem_limit_bytes=62 * 1024 * 1024
        ),
    )(
        tokens, outer_weight, inner_weight, value_weight, mix_out.T, up_weight, down_weight.T,
        conv_taps, norm_first.reshape(1, D), norm_second.reshape(1, D),
    )


def solution(mesh):
    finer = Mesh(
        mesh.devices.reshape(mesh.shape["rep"], 2, 4, 4, mesh.shape["tp"]),
        ("rep", "fs_0", "fs_1", "fs_2", "tp"),
    )
    placed = (
        P(REP_FS_TP, None),
        P(FS, "tp"),
        P(FS, "tp"),
        P(FS, "tp"),
        P(None, "tp"),
        P("tp", FS),
        P(),
        P(FS, "tp"),
        P("tp", FS),
        P(),
    )
    return jax.shard_map(
        local, mesh=finer, in_specs=placed, out_specs=P(REP_FS_TP, None), check_vma=False
    )
```
